32 devices in a mesh: ep: 4 (over y, x), tp: 8 (over z, core).
Axes of the slice: x: 2, y: 2, z: 4, core: 2. Of those that a mesh axis runs over, the one named last changes fastest.
Arguments:
- stream: bfloat16 [64, 2048], P('ep'), may hold values from -6 to 6
- norm_gain_attn: float32 [2048], replicated, may hold values from 0.1 to 1.9
- w_query: bfloat16 [2048, 2048], P('ep', 'tp'), may hold values from -0.125 to 0.125
- w_key: bfloat16 [2048, 2048], P('ep', 'tp'), may hold values from -0.125 to 0.125
- w_value: bfloat16 [2048, 2048], P('ep', 'tp'), may hold values from -0.125 to 0.125
- w_forget: bfloat16 [2048, 16], replicated, may hold values from -0.125 to 0.125
- forget_bias: float32 [16], replicated, may hold values from -2 to 2
- key_cache: bfloat16 [64, 1024, 2048], P('ep', None, 'tp'), may hold values from -1500 to 1500
- value_cache: bfloat16 [64, 1024, 2048], P('ep', None, 'tp'), may hold values from -6 to 6
- gate_cache: float32 [64, 16, 1024], P('ep', 'tp'), may hold values from -1024 to 0, as said below
- lengths: int32 [64], P('ep'), may hold values from 128 to 1024
- w_output: bfloat16 [2048, 2048], P('tp'), may hold values from -0.125 to 0.125
- norm_gain_ffn: float32 [2048], replicated, may hold values from 0.1 to 1.9
- routes: int32 [64, 2], replicated, may hold values from 0 to 3, all different within a row; in each aligned block of 16 rows (0 to 15, 16 to 31, ...) at most 16 rows name the same one
- route_weights: float32 [64, 2], replicated, may hold values from 0.2 to 1
- w_expert_gate: bfloat16 [4, 2048, 5632], P('ep', None, 'tp'), may hold values from -0.125 to 0.125
- w_expert_up: bfloat16 [4, 2048, 5632], P('ep', None, 'tp'), may hold values from -0.125 to 0.125
- expert_down_weight: bfloat16 [4, 5632, 2048], P('ep', 'tp'), may hold values from -0.078125 to 0.078125
Outputs:
- result: bfloat16 [64, 2048], P('ep', 'tp')
The draws below stay inside these ranges and needn't reach their ends.
Inputs may be any that keep to these rules, and one draw needn't show every extreme that they name: `gate_cache`: never rises along positions. `routes`: in the rows of one index of ep no expert is named by more than 16 rows, and in some such block one is named by exactly 16.
All inputs are finite; a program needn't handle non-finite values.
Results may differ from the reference program's by a relative error of at most 0.014.
Values may be sent and summed in bfloat16 or wider, within the bound.
A program may use at most 64 MiB of HBM per device.

```python
import math
import jax
import jax.numpy as jnp
import numpy as np
from jax import lax

D = 2048
HEADS = 16
HEAD_DIM = 128
FF = 5632
TOP = 2
SEQ_DEV = 16
CACHE = 1024
ATT = 2048
BATCH = 64
EXPERTS = 4
CAP = 16
N_EP = 4


def draw_key_cache(key, part):
    parts = jax.random.split(jax.random.fold_in(key, 11), 1)
    base = jax.random.normal(parts[0], (BATCH, CACHE, HEADS, HEAD_DIM), jnp.float32)
    return base.reshape(BATCH, CACHE, HEADS * HEAD_DIM).astype(jnp.bfloat16)


def draw_gate_cache(key, part):
    parts = jax.random.split(jax.random.fold_in(key, 23), 7)
    order = jax.random.permutation(parts[0], HEADS)
    fast_count = HEADS // 2
    fast = (order < fast_count)[None, :, None]
    block_factor = jnp.exp(jax.random.uniform(parts[1], (N_EP, 1, 1), jnp.float32, 0.0, math.log(4.0)))
    seq_factor = jnp.repeat(block_factor, SEQ_DEV, axis=0)
    fast_rate = jnp.exp(jax.random.uniform(parts[2], (BATCH, HEADS, 1), jnp.float32, math.log(1.0 / 50.0), math.log(1.0 / 30.0)))
    slow_rate = jnp.exp(jax.random.uniform(parts[3], (BATCH, HEADS, 1), jnp.float32, math.log(0.5), math.log(1.5))) / CACHE
    rate = jnp.where(fast, fast_rate, slow_rate) * seq_factor
    rough = jax.random.uniform(parts[4], (BATCH, HEADS, CACHE), jnp.float32, 0.0, 2.0)
    generation_iterations = -rate * rough
    sampled_locations = jax.random.randint(parts[5], (BATCH, HEADS, 3), 0, CACHE)
    stack_count = jax.random.uniform(parts[6], (BATCH, HEADS, 3), jnp.float32, math.log(0.5), math.log(0.8))
    sequence_indices = jnp.arange(CACHE)[None, None, None, :]
    clustered_sets = jnp.sum(jnp.where(sequence_indices == sampled_locations[..., None], stack_count[..., None], 0.0), axis=2)
    return jnp.cumsum(generation_iterations + clustered_sets, axis=2)


def touch_ends(drawn, rng, low, high):
    longest = drawn.shape.index(max(drawn.shape))
    spots = []
    for shift in (0, 1):
        where = [jax.random.randint(jax.random.fold_in(rng, axis), (), 0, length) for axis, length in enumerate(drawn.shape)]
        where[longest] = (where[longest] + shift) % drawn.shape[longest]
        spots.append(tuple(where))
    return drawn.at[spots[0]].set(low).at[spots[1]].set(high)


def level_of(own_key, shape, cuts, smallest, high):
    level = 1.0
    for position, blocks in cuts:
        heights = jax.random.uniform(jax.random.fold_in(jax.random.fold_in(own_key, 6), position), (blocks,), jnp.float32, smallest / len(cuts), high / len(cuts))
        level = level * jnp.repeat(jnp.exp(heights), shape[position] // blocks).reshape((-1,) + (1,) * (len(shape) - 1 - position))
    return level


def shared_out(own_key, own, number, rows, amount, top, bound, slope):
    sequence = jax.random.permutation(own_key, amount)
    packed, ordinary = shares(amount, rows * top, bound, slope, True), shares(amount, rows * top, bound, slope, False)
    places = jnp.arange(amount)

    def named(tallies, rotation):
        used = int((tallies > 0).sum())
        fixed = max(1, used // 4)
        moved = fixed + (places - fixed + rotation * (used - fixed)) % max(1, amount - fixed)
        return jnp.zeros((amount,), jnp.int32).at[sequence[jnp.where(places < fixed, places, moved)]].set(jnp.asarray(tallies, jnp.int32))

    tallies = jnp.where(number % 4 == 0, named(packed, number // 4), named(ordinary, number - number // 4 - 1))
    mixed = jax.random.permutation(jax.random.fold_in(own, 3), amount)
    donor, taker = mixed[0:amount // 2 * 2:2], mixed[1:amount // 2 * 2:2]
    margin = jnp.minimum(tallies[donor] - 1, bound - tallies[taker]) // 2
    margin = jnp.where((donor == sequence[0]) | (taker == sequence[0]) | (tallies[taker] == 0), 0, jnp.maximum(margin, 0))
    moved = jax.random.randint(jax.random.fold_in(own, 4), (amount // 2,), 0, 1 << 20) % (margin + 1)
    tallies = tallies.at[donor].add(-moved).at[taker].add(moved)
    items = jnp.searchsorted(jnp.cumsum(tallies), jnp.arange(rows * top), side="right").astype(jnp.int32)
    listing = items.reshape(top, rows).T
    listing = listing[jax.random.permutation(jax.random.fold_in(own, 1), rows)]
    rotation = jax.random.randint(jax.random.fold_in(own, 2), (rows, 1), 0, top)
    return jnp.take_along_axis(listing, (jnp.arange(top)[None, :] + rotation) % top, axis=1)


def shares(number_of, total, most, lean, full):
    portions = [(1 << 20) // math.isqrt(grade ** lean) + 1 for grade in range(1, number_of + 1)]
    largest = most if full else min(most, max(-(-total // number_of), total * portions[0] // sum(portions)))
    least = 1 if total - largest >= number_of - 1 else 0
    counts, spare = [largest] + [least] * (number_of - 1), total - largest - least * (number_of - 1)
    while spare > 0:
        movable = [i for i in range(1, number_of) if counts[i] < largest] or [i for i in range(1, number_of) if counts[i] < most]
        mass, remaining = sum([portions[i] for i in movable]), spare
        for i in movable:
            extra = min(most - counts[i], max(1, remaining * portions[i] // mass), spare)
            counts[i] = counts[i] + extra
            spare = spare - extra
    return np.array(counts)


def scatter_about(own_key, shape, spread, reach, cuts=(), held_as=jnp.bfloat16):
    result = spread * jax.random.normal(own_key, shape, jnp.float32)
    if cuts:
        result = result * level_of(own_key, shape, cuts, -0.22, 0.18)
    return jnp.clip(result, -reach, reach).astype(held_as)


def setup_inputs(seed: int = 0) -> dict:
    key_list = jax.random.split(jax.random.key(seed), 19)
    stream = scatter_about(key_list[0], (BATCH, D), 1.0, 6.0, ((0, 4),))
    norm_gain_attn = jnp.clip(1.0 + 0.18 * jax.random.normal(key_list[1], (D,), jnp.float32), 0.1, 1.9)
    w_query = scatter_about(key_list[2], (D, ATT), D ** -0.5, 0.125, ((0, 4), (1, 8)))
    w_key = scatter_about(key_list[3], (D, ATT), D ** -0.5, 0.125, ((0, 4), (1, 8)))
    w_value = scatter_about(key_list[4], (D, ATT), D ** -0.5, 0.125, ((0, 4), (1, 8)))
    w_forget = scatter_about(key_list[5], (D, HEADS), D ** -0.5, 0.125)
    forget_bias = jnp.clip(jax.random.uniform(key_list[6], (HEADS,), jnp.float32, -2.0, 2.0), -2.0, 2.0)
    key_cache = draw_key_cache(jax.random.fold_in(key_list[18], 71), 0)
    value_cache = scatter_about(key_list[8], (BATCH, CACHE, ATT), 1.0, 6.0, ((0, 4), (2, 8)))
    gate_cache = draw_gate_cache(jax.random.fold_in(key_list[18], 71), 0)
    lengths = touch_ends(jax.random.randint(key_list[10], (BATCH,), CACHE // 8, CACHE + 1), jax.random.fold_in(key_list[10], 1), CACHE // 8, CACHE).astype(jnp.int32)
    w_output = scatter_about(key_list[11], (ATT, D), ATT ** -0.5, 0.125, ((0, 8),))
    norm_gain_ffn = jnp.clip(1.0 + 0.18 * jax.random.normal(key_list[12], (D,), jnp.float32), 0.1, 1.9)
    routes_keys = jax.random.split(jax.random.fold_in(key_list[13], 1), BATCH // SEQ_DEV)
    routes_turns = jax.random.permutation(jax.random.fold_in(key_list[13], 3), BATCH // SEQ_DEV)
    routes = jax.vmap(lambda own, number: shared_out(jax.random.fold_in(key_list[13], 2), own, number, SEQ_DEV, EXPERTS, TOP, CAP, 2))(routes_keys, routes_turns).reshape((BATCH, TOP))
    route_weights = jnp.clip(jax.random.uniform(key_list[14], (BATCH, TOP), jnp.float32, 0.2, 1.0), 0.2, 1.0)
    w_expert_gate = scatter_about(key_list[15], (EXPERTS, D, FF), D ** -0.5, 0.125, ((0, 4), (2, 8)))
    w_expert_up = scatter_about(key_list[16], (EXPERTS, D, FF), D ** -0.5, 0.125, ((0, 4), (2, 8)))
    expert_down_weight = scatter_about(key_list[17], (EXPERTS, FF, D), FF ** -0.5, 0.078125, ((0, 4), (1, 8)))
    return dict(stream=stream, norm_gain_attn=norm_gain_attn, w_query=w_query, w_key=w_key, w_value=w_value, w_forget=w_forget, forget_bias=forget_bias, key_cache=key_cache, value_cache=value_cache, gate_cache=gate_cache, lengths=lengths, w_output=w_output, norm_gain_ffn=norm_gain_ffn, routes=routes, route_weights=route_weights, w_expert_gate=w_expert_gate, w_expert_up=w_expert_up, expert_down_weight=expert_down_weight)


def rms_norm(values, gain):
    floats = values.astype(jnp.float32)
    scaled = floats * lax.rsqrt(lax.optimization_barrier(jnp.mean(floats * floats, axis=-1, keepdims=True)) + 1e-06)
    return (scaled * gain).astype(jnp.bfloat16)

def attend_one(items):
    query, key_new, value_new, forget_new, keys, values, gates, length_total = items
    scale = HEAD_DIM ** (-0.5)
    query_f = query.astype(jnp.float32).reshape(HEADS, HEAD_DIM)
    keys_f = keys.astype(jnp.float32).reshape(CACHE, HEADS, HEAD_DIM)
    value_matrix_float = values.astype(jnp.float32).reshape(CACHE, HEADS, HEAD_DIM)
    sequence_indices = jnp.arange(CACHE, dtype=jnp.int32)
    is_live = sequence_indices < length_total
    last_gate = lax.optimization_barrier(jnp.sum(jnp.where(sequence_indices[None, :] == length_total - 1, gates, 0.0), axis=-1))
    scores = jnp.einsum('hd,phd->hp', query_f, keys_f) * scale + forget_new[:, None] + last_gate[:, None] - gates
    own_score = lax.optimization_barrier(jnp.sum(query_f * key_new.astype(jnp.float32).reshape(HEADS, HEAD_DIM), axis=-1)) * scale
    hidden_from_view = jnp.where(is_live[None, :], scores, -1e+30)
    largest = jnp.maximum(lax.optimization_barrier(jnp.max(hidden_from_view, axis=-1)), own_score)
    past = jnp.exp(hidden_from_view - largest[:, None])
    own_term = jnp.exp(own_score - largest)
    total = lax.optimization_barrier(jnp.sum(past, axis=-1)) + own_term
    past_weights = lax.optimization_barrier((past / total[:, None]).astype(jnp.bfloat16))
    own_weights = lax.optimization_barrier((own_term / total).astype(jnp.bfloat16))
    mixed = jnp.einsum('hp,phd->hd', past_weights.astype(jnp.float32), value_matrix_float)
    mixed = mixed + own_weights.astype(jnp.float32)[:, None] * value_new.astype(jnp.float32).reshape(HEADS, HEAD_DIM)
    return mixed.reshape(HEADS * HEAD_DIM).astype(jnp.bfloat16)

def reference(stream, norm_gain_attn, w_query, w_key, w_value, w_forget, forget_bias, key_cache, value_cache, gate_cache, lengths, w_output, norm_gain_ffn, routes, route_weights, w_expert_gate, w_expert_up, expert_down_weight):
    normed = rms_norm(stream, norm_gain_attn)
    query = jnp.dot(normed, w_query, preferred_element_type=jnp.float32).astype(jnp.bfloat16)
    key_new = jnp.dot(normed, w_key, preferred_element_type=jnp.float32).astype(jnp.bfloat16)
    value_new = jnp.dot(normed, w_value, preferred_element_type=jnp.float32).astype(jnp.bfloat16)
    forget_new = jax.nn.log_sigmoid(jnp.dot(normed, w_forget, preferred_element_type=jnp.float32) + forget_bias)
    attended = lax.map(attend_one, (query, key_new, value_new, forget_new, key_cache, value_cache, gate_cache, lengths))
    mixed = (stream.astype(jnp.float32) + jnp.dot(attended, w_output, preferred_element_type=jnp.float32)).astype(jnp.bfloat16)
    normed_ffn = rms_norm(mixed, norm_gain_ffn)
    flat_routes = routes.reshape(-1)
    flat_weights = route_weights.reshape(-1)
    owners = (jnp.arange(BATCH * TOP, dtype=jnp.int32) // TOP).astype(jnp.int32)
    slot_numbers = jnp.arange(CAP * N_EP, dtype=jnp.int32)

    def expert_step(combined, items):
        gate_w, up_w, down_w, index = items
        chosen = flat_routes == index
        chosen_count = jnp.sum(chosen.astype(jnp.int32))
        picks = jnp.nonzero(chosen, size=CAP * N_EP, fill_value=0)[0].astype(jnp.int32)
        token_ids = owners[picks]
        inputs = normed_ffn[token_ids]
        hidden = (jax.nn.silu(jnp.dot(inputs, gate_w, preferred_element_type=jnp.float32)) * jnp.dot(inputs, up_w, preferred_element_type=jnp.float32)).astype(jnp.bfloat16)
        outputs = lax.optimization_barrier(jnp.dot(hidden, down_w, preferred_element_type=jnp.float32).astype(jnp.bfloat16))
        weights = jnp.where(slot_numbers < chosen_count, flat_weights[picks], 0.0)
        return (combined.at[token_ids].add(outputs.astype(jnp.float32) * weights[:, None]), None)
    combined, _ = lax.scan(expert_step, jnp.zeros((BATCH, D), jnp.float32), (w_expert_gate, w_expert_up, expert_down_weight, jnp.arange(EXPERTS, dtype=jnp.int32)))
    return (mixed.astype(jnp.float32) + combined).astype(jnp.bfloat16)
```

```python
import functools

import jax
import jax.numpy as jnp
from jax import lax
from jax.experimental import pallas as pl
from jax.experimental.pallas import tpu as pltpu
from jax.sharding import PartitionSpec as P

F32 = jnp.float32
BF16 = jnp.bfloat16
DOWN_GROUPS = 4
SEQ_GROUPS = 2
CACHE_LOADS = 4
LANES = 128


def inverse_rms(floats):
    return lax.rsqrt(jnp.mean(floats * floats, axis=-1, keepdims=True) + 1e-06)


def matmul(a, b):
    return jnp.dot(a, b, preferred_element_type=F32)


def matmul_t(a, b):
    return lax.dot_general(a, b, (((1,), (1,)), ((), ())), preferred_element_type=F32)


def flip(index, bits):
    moved, bit = index, 1
    while bit <= bits:
        if bits & bit:
            moved = moved + bit - 2 * bit * lax.rem(lax.div(index, bit), 2)
        bit *= 2
    return moved


def layer_kernel(
    n_ep,
    n_tp,
    heads,
    stream_hbm,
    gain_attn_hbm,
    w_forget_hbm,
    forget_bias_hbm,
    gates_hbm,
    lengths_hbm,
    gain_ffn_hbm,
    routes_hbm,
    route_weights_hbm,
    wq_hbm,
    wk_hbm,
    wv_hbm,
    keys_hbm,
    values_hbm,
    wo_hbm,
    wg_hbm,
    wu_hbm,
    wd_hbm,
    out,
    stream,
    gain_attn,
    w_forget,
    forget_bias,
    gates,
    lengths,
    gain_ffn,
    routes,
    route_weights,
    wqkv,
    keys,
    keys_t,
    values,
    wo,
    wg,
    wu,
    wd,
    wg_t,
    wu_t,
    a2a_send,
    a2a_recv,
    part_send,
    part_recv,
    gate_rows,
    pair_send,
    pair_recv,
    own_part,
    zs_send,
    zs_recv,
    mix,
    dn_send,
    dn_recv,
    fs_send,
    fs_recv,
    small_sem,
    w_sem,
    k_sem,
    v_sem,
    a2a_ss,
    a2a_rs,
    part_ss,
    part_rs,
    pair_ss,
    pair_rs,
    zs_ss,
    zs_rs,
    mix_ss,
    mix_rs,
    dn_ss,
    dn_rs,
    fs_ss,
    fs_rs,
):
    my_ep = lax.axis_index("ep")
    my_tp = lax.axis_index("tp")
    seqs, width = stream.shape
    depth = wq_hbm.shape[0]
    cols = wq_hbm.shape[1]
    cache = keys.shape[1]
    head_dim = cols // heads
    slice_w = out.shape[1]
    hidden_w = wg_hbm.shape[1]
    tokens = n_ep * seqs
    levels = n_tp // 2
    half_w = levels * slice_w
    core, level = lax.rem(my_tp, 2), lax.div(my_tp, 2)
    sg = seqs // SEQ_GROUPS
    grows = heads * sg
    rows = SEQ_GROUPS * grows

    def ep_at(k):
        return flip(my_ep, k)

    def tp_at(d):
        return flip(my_tp, d)

    def remote(src, dst, ss, rs, device):
        return pltpu.make_async_remote_copy(
            src_ref=src,
            dst_ref=dst,
            send_sem=ss,
            recv_sem=rs,
            device_id=device,
            device_id_type=pl.DeviceIdType.MESH,
        )

    barrier = pltpu.get_barrier_semaphore()
    for c in range(2):
        for k in range(1, n_ep):
            pl.semaphore_signal(
                barrier,
                inc=1,
                device_id={"ep": ep_at(k), "tp": tp_at(c)},
                device_id_type=pl.DeviceIdType.MESH,
            )
    for d in range(1, n_tp):
        pl.semaphore_signal(
            barrier, inc=1, device_id={"tp": tp_at(d)}, device_id_type=pl.DeviceIdType.MESH
        )

    small = [
        pltpu.make_async_copy(src, dst, small_sem.at[i])
        for i, (src, dst) in enumerate(
            (
                (stream_hbm, stream),
                (gain_attn_hbm, gain_attn),
                (w_forget_hbm, w_forget),
                (forget_bias_hbm, forget_bias),
                (gates_hbm, gates),
                (lengths_hbm, lengths),
                (gain_ffn_hbm, gain_ffn),
                (routes_hbm, routes),
                (route_weights_hbm, route_weights),
            )
        )
    ]
    loads = [
        pltpu.make_async_copy(src, dst, w_sem.at[i])
        for i, (src, dst) in enumerate(
            (
                (wq_hbm, wqkv.at[0]),
                (wk_hbm, wqkv.at[1]),
                (wv_hbm, wqkv.at[2]),
                (wo_hbm, wo),
                (wg_hbm.at[0], wg.at[pl.ds(0, hidden_w)]),
                (wu_hbm.at[0], wu.at[pl.ds(0, hidden_w)]),
                (wd_hbm.at[0], wd.at[pl.ds(0, hidden_w)]),
            )
        )
    ]
    span = seqs // CACHE_LOADS
    key_loads = [
        pltpu.make_async_copy(
            keys_hbm.at[pl.ds(i * span, span)], keys.at[pl.ds(i * span, span)], k_sem.at[i]
        )
        for i in range(CACHE_LOADS)
    ]
    value_loads = [
        pltpu.make_async_copy(
            values_hbm.at[pl.ds(i * span, span)], values.at[pl.ds(i * span, span)], v_sem.at[i]
        )
        for i in range(CACHE_LOADS)
    ]
    for load in small[:2] + loads[:3] + small[2:]:
        load.start()
    for load in key_loads + value_loads + loads[3:]:
        load.start(priority=1)

    spare = wg.shape[0] - hidden_w
    if spare:
        for w in (wg, wu, wd):
            w[hidden_w:, :] = jnp.zeros((spare, width), BF16)

    small[0].wait()
    small[1].wait()
    floats = stream[...].astype(F32)
    normed = (floats * inverse_rms(floats) * gain_attn[...]).astype(BF16)
    for e in range(n_ep):
        a2a_send[e] = normed[:, e * depth : (e + 1) * depth]

    pl.semaphore_wait(barrier, 2 * (n_ep - 1) + n_tp - 1)

    sent = []
    a2a = []
    for k in reversed(range(1, n_ep)):
        copy = remote(
            a2a_send.at[ep_at(k)], a2a_recv.at[my_ep], a2a_ss.at[k], a2a_rs.at[k], {"ep": ep_at(k)}
        )
        copy.start()
        a2a.append(copy)
    sent += a2a
    a2a_recv[my_ep] = a2a_send[my_ep]

    for load in small[2:]:
        load.wait()
    forget_all = matmul_t(normed, w_forget[...]) + forget_bias[...]
    forget_all = -(jnp.maximum(-forget_all, 0.0) + jnp.log1p(jnp.exp(-jnp.abs(forget_all))))
    head_lane = lax.broadcasted_iota(jnp.int32, (sg, forget_all.shape[1]), 1)
    forget_new = jnp.concatenate(
        [
            jnp.sum(
                jnp.where(
                    head_lane == my_tp * heads + h, forget_all[g * sg : (g + 1) * sg], 0.0
                ),
                axis=1,
                keepdims=True,
            )
            for g in range(SEQ_GROUPS)
            for h in range(heads)
        ],
        axis=0,
    )
    for g in range(SEQ_GROUPS):
        for h in range(heads):
            for s in range(sg):
                r = (g * heads + h) * sg + s
                gate_rows[r : r + 1, :] = gates[g * sg + s, h : h + 1, :]
    row = lax.broadcasted_iota(jnp.int32, (rows, seqs), 0)
    row_seq = row // grows * sg + row % sg
    length_f = lengths[...].astype(F32)
    live_count = jnp.sum(
        jnp.where(lax.broadcasted_iota(jnp.int32, (rows, seqs), 1) == row_seq, length_f, 0.0),
        axis=1,
        keepdims=True,
    ).astype(jnp.int32)
    position = lax.broadcasted_iota(jnp.int32, (rows, cache), 1)
    last_gate = jnp.sum(
        jnp.where(position == live_count - 1, gate_rows[...], 0.0), axis=1, keepdims=True
    )
    gate_rows[...] = jnp.where(
        position < live_count, forget_new + (last_gate - gate_rows[...]), -1e30
    )

    for load in loads[:3]:
        load.wait()
    for copy in a2a:
        copy.wait_recv()
    block = a2a_recv[...].reshape(tokens, depth)
    parts = []
    for i in range(3):
        product = matmul(block, wqkv[i])
        for e in range(n_ep):
            part_send[i, e] = product[e * seqs : (e + 1) * seqs]
        step = []
        for k in reversed(range(1, n_ep)):
            copy = remote(
                part_send.at[i, ep_at(k)],
                part_recv.at[i, my_ep],
                part_ss.at[i, k],
                part_rs.at[i, k],
                {"ep": ep_at(k)},
            )
            copy.start()
            step.append(copy)
        parts.append(step)
        sent += step
        part_recv[i, my_ep] = part_send[i, my_ep]

    for i in range(CACHE_LOADS):
        key_loads[i].wait()

        @pl.loop(i * span, (i + 1) * span)
        def _(s):
            keys_t[pl.ds(pl.multiple_of(s * cols, cols), cols), :] = keys[s].T

    def projected(i):
        for copy in parts[i]:
            copy.wait_recv()
        total = part_recv[i, 0]
        for e in range(1, n_ep):
            total = total + part_recv[i, e]
        return total.astype(BF16).astype(F32)

    scale = head_dim ** (-0.5)
    query = projected(0)
    lane_head = lax.broadcasted_iota(jnp.int32, (sg, cols), 1) // head_dim
    group_seq = lax.broadcasted_iota(jnp.int32, (grows, 1), 0) % sg

    def by_head(values_of):
        return jnp.concatenate(values_of, axis=0)

    def score(g):
        mine = query[g * sg : (g + 1) * sg]
        spread = by_head([jnp.where(lane_head == h, mine, 0.0) for h in range(heads)])
        lhs = jnp.concatenate(
            [jnp.where(group_seq == s, spread, 0.0).astype(BF16) for s in range(sg)], axis=1
        )
        return matmul(lhs, keys_t[g * sg * cols : (g + 1) * sg * cols, :])

    def finish_pair(g):
        pairs[g].wait_recv()
        zs_send[g] = (own_part[g] + pair_recv[g].astype(F32)).astype(BF16)
        step = []
        for d in reversed(range(1, levels)):
            copy = remote(
                zs_send.at[g], zs_recv.at[g, d], zs_ss.at[g, d], zs_rs.at[g, d], {"tp": tp_at(2 * d)}
            )
            copy.start()
            step.append(copy)
        zsum.append(step)
        sent.extend(step)

    pairs, zsum = [], []
    for g in range(SEQ_GROUPS):
        found = score(g)
        if g == 0:
            key_new = projected(1)
            value_new = projected(2)
        mine = slice(g * sg, (g + 1) * sg)
        own_score = (
            by_head(
                [
                    jnp.sum(
                        jnp.where(lane_head == h, query[mine] * key_new[mine], 0.0),
                        axis=1,
                        keepdims=True,
                    )
                    for h in range(heads)
                ]
            )
            * scale
        )
        full = found * scale + gate_rows[g * grows : (g + 1) * grows, :]
        largest = jnp.maximum(jnp.max(full, axis=1, keepdims=True), own_score)
        past = jnp.exp(full - largest)
        own_term = jnp.exp(own_score - largest)
        total = jnp.sum(past, axis=1, keepdims=True) + own_term
        past_weights = past / total
        own_weight = (own_term / total).astype(BF16).astype(F32)
        if g:
            finish_pair(g - 1)
        for i in range(CACHE_LOADS):
            if i * span // sg == g:
                value_loads[i].wait()
        gathered = jnp.zeros((grows, cols), F32)
        for s in range(sg):
            chosen = jnp.where(group_seq == s, past_weights, 0.0).astype(BF16)
            gathered = gathered + matmul(chosen, values[g * sg + s])
        attended = jnp.zeros((sg, cols), F32)
        for h in range(heads):
            part = slice(h * sg, (h + 1) * sg)
            attended = jnp.where(
                lane_head == h, gathered[part] + own_weight[part] * value_new[mine], attended
            )
        attended = attended.astype(BF16)
        if g == 0:
            loads[3].wait()

        def outward(c):
            return jnp.concatenate(
                [
                    matmul(
                        attended,
                        wo[:, pl.ds(pl.multiple_of((2 * t + c) * slice_w, slice_w), slice_w)],
                    )
                    for t in range(levels)
                ],
                axis=1,
            )

        pair_send[g] = outward(1 - core).astype(BF16)
        copy = remote(
            pair_send.at[g], pair_recv.at[g], pair_ss.at[g], pair_rs.at[g], {"tp": tp_at(1)}
        )
        copy.start()
        pairs.append(copy)
        sent.append(copy)
        own_part[g] = outward(core)
    finish_pair(SEQ_GROUPS - 1)

    stream_half = jnp.concatenate(
        [
            stream[:, pl.ds(pl.multiple_of((2 * t + core) * slice_w, slice_w), slice_w)]
            for t in range(levels)
        ],
        axis=1,
    ).astype(F32)

    def transposed(src, dst):
        @pl.loop(0, n_tp)
        def _(t):
            into = lax.rem(t, 2) * half_w + lax.div(t, 2) * slice_w
            dst[pl.ds(pl.multiple_of(into, slice_w), slice_w), :] = src[
                :, pl.ds(pl.multiple_of(t * slice_w, slice_w), slice_w)
            ].T

    mixes = []
    for g in range(SEQ_GROUPS):
        if g < 2:
            loads[4 + g].wait()
            transposed(*((wg, wg_t), (wu, wu_t))[g])
        total = stream_half[g * sg : (g + 1) * sg] + zs_send[g].astype(F32)
        for d in range(1, levels):
            zsum[g][-d].wait_recv()
            total = total + zs_recv[g, d].astype(F32)
        mix[core, my_ep, g] = total.astype(BF16)
        here = mix.at[core, my_ep, g]
        step = []
        for k in reversed(range(n_ep)):
            for c in range(2):
                if k or c:
                    copy = remote(
                        here,
                        here,
                        mix_ss.at[g, k, c],
                        mix_rs.at[g, k, c],
                        {"ep": ep_at(k), "tp": tp_at(c)},
                    )
                    copy.start()
                    step.append(copy)
        mixes += step
    sent += mixes

    share = jnp.sum(
        jnp.where(routes[...] == my_ep, route_weights[...], 0.0), axis=0, keepdims=True
    )
    square = (tokens, tokens)
    diagonal = lax.broadcasted_iota(jnp.int32, square, 0) == lax.broadcasted_iota(
        jnp.int32, square, 1
    )
    coefficient = jnp.sum(jnp.where(diagonal, share, 0.0), axis=1, keepdims=True)
    loads[6].wait()
    for copy in mixes:
        copy.wait_recv()
    halves = [mix[c].astype(F32).reshape(tokens, half_w) for c in range(2)]
    squares = sum(jnp.sum(half * half, axis=1, keepdims=True) for half in halves)
    inverse = lax.rsqrt(squares / width + 1e-06)
    normed_ffn = jnp.concatenate(
        [
            (
                halves[c]
                * inverse
                * jnp.concatenate(
                    [
                        gain_ffn[:, (2 * t + c) * slice_w : (2 * t + c + 1) * slice_w]
                        for t in range(levels)
                    ],
                    axis=1,
                )
            ).astype(BF16)
            for c in range(2)
        ],
        axis=1,
    )
    gate = matmul(normed_ffn, wg_t[...])
    up = matmul(normed_ffn, wu_t[...])
    hidden = (gate / (1.0 + jnp.exp(-gate)) * up).astype(BF16)

    down = []
    size = n_tp // DOWN_GROUPS
    for g in reversed(range(DOWN_GROUPS)):
        for d in reversed(range(g * size, (g + 1) * size)):
            at = pl.ds(pl.multiple_of(tp_at(d) * slice_w, slice_w), slice_w)
            product = (matmul(hidden, wd[:, at]) * coefficient).astype(BF16)
            for e in range(n_ep):
                dn_send[e, d] = product[e * seqs : (e + 1) * seqs]
        step = []
        group = pl.ds(g * size, size)
        for k in reversed(range(1, n_ep)):
            copy = remote(
                dn_send.at[ep_at(k), group],
                dn_recv.at[k, group],
                dn_ss.at[g, k],
                dn_rs.at[g, k],
                {"ep": ep_at(k)},
            )
            copy.start()
            step.append(copy)
        down.append(step)
        sent += step
    final = []
    for d in reversed(range(n_tp)):
        if d % size == size - 1:
            for copy in down[DOWN_GROUPS - 1 - d // size]:
                copy.wait_recv()
        summed = dn_send[my_ep, d].astype(F32)
        for k in range(1, n_ep):
            summed = summed + dn_recv[k, d].astype(F32)
        if d:
            fs_send[d] = summed.astype(BF16)
            copy = remote(fs_send.at[d], fs_recv.at[d], fs_ss.at[d], fs_rs.at[d], {"tp": tp_at(d)})
            copy.start()
            final.append(copy)
    sent += final
    combined = summed
    own_stream = mix[
        core, my_ep, :, :, pl.ds(pl.multiple_of(level * slice_w, slice_w), slice_w)
    ].astype(F32).reshape(seqs, slice_w)
    combined = own_stream + combined
    for d in range(1, n_tp):
        final[-d].wait_recv()
        combined = combined + fs_recv[d].astype(F32)
    out[...] = combined.astype(BF16)
    for copy in sent:
        copy.wait_send()


def shards(
    stream,
    norm_gain_attn,
    w_query,
    w_key,
    w_value,
    w_forget,
    forget_bias,
    key_cache,
    value_cache,
    gate_cache,
    lengths,
    w_output,
    norm_gain_ffn,
    routes,
    route_weights,
    w_expert_gate,
    w_expert_up,
    expert_down_weight,
):
    n_ep = lax.axis_size("ep")
    n_tp = lax.axis_size("tp")
    seqs, width = stream.shape
    heads = gate_cache.shape[1]
    cache = key_cache.shape[1]
    depth, cols = w_query.shape
    hidden = w_expert_gate.shape[2]
    padded = -(-hidden // LANES) * LANES
    slice_w = width // n_tp
    levels = n_tp // 2
    half_w = levels * slice_w
    rows = heads * seqs
    sg = seqs // SEQ_GROUPS
    vmem = pl.BlockSpec(memory_space=pltpu.VMEM)
    hbm = pl.BlockSpec(memory_space=pltpu.HBM)
    dma = pltpu.SemaphoreType.DMA
    small = (
        stream,
        norm_gain_attn[None, :],
        w_forget.T,
        forget_bias[None, :],
        gate_cache,
        lengths[None, :],
        norm_gain_ffn[None, :],
        routes.T,
        route_weights.T,
    )
    return pl.pallas_call(
        functools.partial(layer_kernel, n_ep, n_tp, heads),
        out_shape=jax.ShapeDtypeStruct((seqs, slice_w), BF16),
        in_specs=[hbm] * 18,
        out_specs=vmem,
        scratch_shapes=[pltpu.VMEM(array.shape, array.dtype) for array in small]
        + [
            pltpu.VMEM((3, depth, cols), BF16),
            pltpu.VMEM((seqs, cache, cols), BF16),
            pltpu.VMEM((seqs * cols, cache), BF16),
            pltpu.VMEM((seqs, cache, cols), BF16),
            pltpu.VMEM((cols, width), BF16),
            pltpu.VMEM((padded, width), BF16),
            pltpu.VMEM((padded, width), BF16),
            pltpu.VMEM((padded, width), BF16),
            pltpu.VMEM((width, padded), BF16),
            pltpu.VMEM((width, padded), BF16),
            pltpu.VMEM((n_ep, seqs, depth), BF16),
            pltpu.VMEM((n_ep, seqs, depth), BF16),
            pltpu.VMEM((3, n_ep, seqs, cols), F32),
            pltpu.VMEM((3, n_ep, seqs, cols), F32),
            pltpu.VMEM((rows, cache), F32),
            pltpu.VMEM((SEQ_GROUPS, sg, half_w), BF16),
            pltpu.VMEM((SEQ_GROUPS, sg, half_w), BF16),
            pltpu.VMEM((SEQ_GROUPS, sg, half_w), F32),
            pltpu.VMEM((SEQ_GROUPS, sg, half_w), BF16),
            pltpu.VMEM((SEQ_GROUPS, levels, sg, half_w), BF16),
            pltpu.VMEM((2, n_ep, SEQ_GROUPS, sg, half_w), BF16),
            pltpu.VMEM((n_ep, n_tp, seqs, slice_w), BF16),
            pltpu.VMEM((n_ep, n_tp, seqs, slice_w), BF16),
            pltpu.VMEM((n_tp, seqs, slice_w), BF16),
            pltpu.VMEM((n_tp, seqs, slice_w), BF16),
            dma((len(small),)),
            dma((7,)),
            dma((CACHE_LOADS,)),
            dma((CACHE_LOADS,)),
            dma((n_ep,)),
            dma((n_ep,)),
            dma((3, n_ep)),
            dma((3, n_ep)),
            dma((SEQ_GROUPS,)),
            dma((SEQ_GROUPS,)),
            dma((SEQ_GROUPS, levels)),
            dma((SEQ_GROUPS, levels)),
            dma((SEQ_GROUPS, n_ep, 2)),
            dma((SEQ_GROUPS, n_ep, 2)),
            dma((DOWN_GROUPS, n_ep)),
            dma((DOWN_GROUPS, n_ep)),
            dma((n_tp,)),
            dma((n_tp,)),
        ],
        compiler_params=pltpu.CompilerParams(
            collective_id=0, has_side_effects=True, vmem_limit_bytes=56 * 1024 * 1024
        ),
    )(
        *small,
        w_query,
        w_key,
        w_value,
        key_cache,
        value_cache,
        w_output,
        jnp.swapaxes(w_expert_gate, 1, 2),
        jnp.swapaxes(w_expert_up, 1, 2),
        expert_down_weight,
    )


def solution(mesh):
    placed = (
        P("ep", None),
        P(),
        P("ep", "tp"),
        P("ep", "tp"),
        P("ep", "tp"),
        P(),
        P(),
        P("ep", None, "tp"),
        P("ep", None, "tp"),
        P("ep", "tp", None),
        P("ep"),
        P("tp", None),
        P(),
        P(),
        P(),
        P("ep", None, "tp"),
        P("ep", None, "tp"),
        P("ep", "tp", None),
    )
    return jax.shard_map(
        shards, mesh=mesh, in_specs=placed, out_specs=P("ep", "tp"), check_vma=False
    )
```

```python
import functools

import jax
import jax.numpy as jnp
from jax import lax
from jax.experimental import pallas as pl
from jax.experimental.pallas import tpu as pltpu
from jax.sharding import PartitionSpec as P

F32 = jnp.float32
BF16 = jnp.bfloat16
SEQ_GROUPS = 2
CACHE_LOADS = 4
LANES = 128


def inverse_rms(floats):
    return lax.rsqrt(jnp.mean(floats * floats, axis=-1, keepdims=True) + 1e-06)


def matmul(a, b):
    return jnp.dot(a, b, preferred_element_type=F32)


def matmul_t(a, b):
    return lax.dot_general(a, b, (((1,), (1,)), ((), ())), preferred_element_type=F32)


def flip(index, bits):
    moved, bit = index, 1
    while bit <= bits:
        if bits & bit:
            moved = moved + bit - 2 * bit * lax.rem(lax.div(index, bit), 2)
        bit *= 2
    return moved


def layer_kernel(
    n_ep,
    n_tp,
    heads,
    stream_hbm,
    gain_attn_hbm,
    w_forget_hbm,
    forget_bias_hbm,
    gates_hbm,
    lengths_hbm,
    gain_ffn_hbm,
    routes_hbm,
    route_weights_hbm,
    wq_hbm,
    wk_hbm,
    wv_hbm,
    keys_hbm,
    values_hbm,
    wo_hbm,
    wg_hbm,
    wu_hbm,
    wd_hbm,
    out,
    stream,
    gain_attn,
    w_forget,
    forget_bias,
    gates,
    lengths,
    gain_ffn,
    routes,
    route_weights,
    wqkv,
    keys,
    keys_t,
    values,
    wo,
    wg,
    wu,
    wd,
    wg_t,
    wu_t,
    a2a_send,
    a2a_recv,
    part_send,
    part_recv,
    gate_rows,
    pair_send,
    pair_recv,
    own_part,
    zs_send,
    zs_recv,
    mix,
    dpair_send,
    dpair_recv,
    down_part,
    fs_send,
    fs_recv,
    small_sem,
    w_sem,
    k_sem,
    v_sem,
    relay,
    a2a_ss,
    a2a_rs,
    part_ss,
    part_rs,
    pair_ss,
    pair_rs,
    zs_ss,
    zs_rs,
    mix_ss,
    mix_rs,
    dpair_ss,
    dpair_rs,
    fs_ss,
    fs_rs,
):
    my_ep = lax.axis_index("ep")
    my_tp = lax.axis_index("tp")
    seqs, width = stream.shape
    depth = wq_hbm.shape[0]
    cols = wq_hbm.shape[1]
    cache = keys.shape[1]
    head_dim = cols // heads
    slice_w = out.shape[1]
    hidden_w = wg_hbm.shape[1]
    tokens = n_ep * seqs
    levels = n_tp // 2
    half_w = levels * slice_w
    core, level = lax.rem(my_tp, 2), lax.div(my_tp, 2)
    sg = seqs // SEQ_GROUPS
    grows = heads * sg
    rows = SEQ_GROUPS * grows

    def ep_at(k):
        return flip(my_ep, k)

    def tp_at(d):
        return flip(my_tp, d)

    def remote(src, dst, ss, rs, device):
        return pltpu.make_async_remote_copy(
            src_ref=src,
            dst_ref=dst,
            send_sem=ss,
            recv_sem=rs,
            device_id=device,
            device_id_type=pl.DeviceIdType.MESH,
        )

    def wait_all(ref, sem):
        pltpu.make_async_copy(ref, ref, sem).wait()

    others = pl.ds(1, n_ep - 1)
    barrier = pltpu.get_barrier_semaphore()
    bits = [1 << b for b in range(levels.bit_length() - 1)]
    met = [{"ep": ep_at(k)} for k in reversed(range(1, n_ep))]
    met += [{"tp": tp_at(1)}] + [{"tp": tp_at(2 * b)} for b in bits]
    for device in met:
        pl.semaphore_signal(barrier, inc=1, device_id=device, device_id_type=pl.DeviceIdType.MESH)

    small = [
        pltpu.make_async_copy(src, dst, small_sem.at[i])
        for i, (src, dst) in enumerate(
            (
                (stream_hbm, stream),
                (gain_attn_hbm, gain_attn),
                (w_forget_hbm, w_forget),
                (forget_bias_hbm, forget_bias),
                (gates_hbm, gates),
                (lengths_hbm, lengths),
                (gain_ffn_hbm, gain_ffn),
                (routes_hbm, routes),
                (route_weights_hbm, route_weights),
            )
        )
    ]
    loads = [
        pltpu.make_async_copy(src, dst, w_sem.at[i])
        for i, (src, dst) in enumerate(
            (
                (wq_hbm, wqkv.at[0]),
                (wk_hbm, wqkv.at[1]),
                (wv_hbm, wqkv.at[2]),
                (wo_hbm, wo),
                (wg_hbm.at[0], wg.at[pl.ds(0, hidden_w)]),
                (wu_hbm.at[0], wu.at[pl.ds(0, hidden_w)]),
                (wd_hbm.at[0], wd.at[pl.ds(0, hidden_w)]),
            )
        )
    ]
    span = seqs // CACHE_LOADS
    key_loads = [
        pltpu.make_async_copy(
            keys_hbm.at[pl.ds(i * span, span)], keys.at[pl.ds(i * span, span)], k_sem.at[i]
        )
        for i in range(CACHE_LOADS)
    ]
    value_loads = [
        pltpu.make_async_copy(
            values_hbm.at[pl.ds(i * span, span)], values.at[pl.ds(i * span, span)], v_sem.at[i]
        )
        for i in range(CACHE_LOADS)
    ]
    for load in small[:2] + loads[:3] + small[2:]:
        load.start()
    for load in key_loads + value_loads + loads[3:]:
        load.start(priority=1)

    spare = wg.shape[0] - hidden_w
    if spare:
        for w in (wg, wu, wd):
            w[hidden_w:, :] = jnp.zeros((spare, width), BF16)

    small[0].wait()
    small[1].wait()
    floats = stream[...].astype(F32)
    normed = (floats * inverse_rms(floats) * gain_attn[...]).astype(BF16)
    for e in range(n_ep):
        a2a_send[e] = normed[:, e * depth : (e + 1) * depth]

    pl.semaphore_wait(barrier, len(met))

    for k in reversed(range(1, n_ep)):
        remote(a2a_send.at[ep_at(k)], a2a_recv.at[k], a2a_ss, a2a_rs, {"ep": ep_at(k)}).start()
    a2a_recv[0] = a2a_send[my_ep]
    for i, b in enumerate(bits[:-1]):
        pl.semaphore_signal(
            relay.at[i],
            inc=1,
            device_id={"tp": tp_at(2 * b)},
            device_id_type=pl.DeviceIdType.MESH,
        )
        pl.semaphore_wait(relay.at[i], 1)

    for load in small[2:]:
        load.wait()
    forget_all = matmul_t(normed, w_forget[...]) + forget_bias[...]
    forget_all = -(jnp.maximum(-forget_all, 0.0) + jnp.log1p(jnp.exp(-jnp.abs(forget_all))))
    head_lane = lax.broadcasted_iota(jnp.int32, (sg, forget_all.shape[1]), 1)
    forget_new = jnp.concatenate(
        [
            jnp.sum(
                jnp.where(
                    head_lane == my_tp * heads + h, forget_all[g * sg : (g + 1) * sg], 0.0
                ),
                axis=1,
                keepdims=True,
            )
            for g in range(SEQ_GROUPS)
            for h in range(heads)
        ],
        axis=0,
    )
    for g in range(SEQ_GROUPS):
        for h in range(heads):
            for s in range(sg):
                r = (g * heads + h) * sg + s
                gate_rows[r : r + 1, :] = gates[g * sg + s, h : h + 1, :]
    row = lax.broadcasted_iota(jnp.int32, (rows, seqs), 0)
    row_seq = row // grows * sg + row % sg
    length_f = lengths[...].astype(F32)
    live_count = jnp.sum(
        jnp.where(lax.broadcasted_iota(jnp.int32, (rows, seqs), 1) == row_seq, length_f, 0.0),
        axis=1,
        keepdims=True,
    ).astype(jnp.int32)
    position = lax.broadcasted_iota(jnp.int32, (rows, cache), 1)
    last_gate = jnp.sum(
        jnp.where(position == live_count - 1, gate_rows[...], 0.0), axis=1, keepdims=True
    )
    gate_rows[...] = jnp.where(
        position < live_count, forget_new + (last_gate - gate_rows[...]), -1e30
    )

    for load in loads[:3]:
        load.wait()
    wait_all(a2a_recv.at[others], a2a_rs)
    block = a2a_recv[...].reshape(tokens, depth)
    for i in range(3):
        product = matmul(block, wqkv[i])
        for k in reversed(range(1, n_ep)):
            part_send[i, k] = product[k * seqs : (k + 1) * seqs]
            remote(
                part_send.at[i, k], part_recv.at[i, k], part_ss, part_rs.at[i], {"ep": ep_at(k)}
            ).start()
        part_recv[i, 0] = product[:seqs]

    for i in range(CACHE_LOADS):
        key_loads[i].wait()

        @pl.loop(i * span, (i + 1) * span)
        def _(s):
            keys_t[pl.ds(pl.multiple_of(s * cols, cols), cols), :] = keys[s].T

    def projected(i):
        wait_all(part_recv.at[i, others], part_rs.at[i])
        total = part_recv[i, 0]
        for e in range(1, n_ep):
            total = total + part_recv[i, e]
        return total.astype(BF16).astype(F32)

    scale = head_dim ** (-0.5)
    query = projected(0)
    lane_head = lax.broadcasted_iota(jnp.int32, (sg, cols), 1) // head_dim
    group_seq = lax.broadcasted_iota(jnp.int32, (grows, 1), 0) % sg

    def by_head(values_of):
        return jnp.concatenate(values_of, axis=0)

    def score(g):
        mine = query[g * sg : (g + 1) * sg]
        spread = by_head([jnp.where(lane_head == h, mine, 0.0) for h in range(heads)])
        lhs = jnp.concatenate(
            [jnp.where(group_seq == s, spread, 0.0).astype(BF16) for s in range(sg)], axis=1
        )
        return matmul(lhs, keys_t[g * sg * cols : (g + 1) * sg * cols, :])

    def finish_pair(g):
        wait_all(pair_recv.at[g], pair_rs.at[g])
        zs_send[g] = (own_part[g] + pair_recv[g].astype(F32)).astype(BF16)
        for d in reversed(range(1, levels)):
            remote(
                zs_send.at[g], zs_recv.at[g, d], zs_ss, zs_rs.at[g], {"tp": tp_at(2 * d)}
            ).start()

    for g in range(SEQ_GROUPS):
        found = score(g)
        if g == 0:
            key_new = projected(1)
            value_new = projected(2)
        mine = slice(g * sg, (g + 1) * sg)
        own_score = (
            by_head(
                [
                    jnp.sum(
                        jnp.where(lane_head == h, query[mine] * key_new[mine], 0.0),
                        axis=1,
                        keepdims=True,
                    )
                    for h in range(heads)
                ]
            )
            * scale
        )
        full = found * scale + gate_rows[g * grows : (g + 1) * grows, :]
        largest = jnp.maximum(jnp.max(full, axis=1, keepdims=True), own_score)
        past = jnp.exp(full - largest)
        own_term = jnp.exp(own_score - largest)
        total = jnp.sum(past, axis=1, keepdims=True) + own_term
        past_weights = past / total
        own_weight = (own_term / total).astype(BF16).astype(F32)
        if g:
            finish_pair(g - 1)
        for i in range(CACHE_LOADS):
            if i * span // sg == g:
                value_loads[i].wait()
        gathered = jnp.zeros((grows, cols), F32)
        for s in range(sg):
            chosen = jnp.where(group_seq == s, past_weights, 0.0).astype(BF16)
            gathered = gathered + matmul(chosen, values[g * sg + s])
        attended = jnp.zeros((sg, cols), F32)
        for h in range(heads):
            part = slice(h * sg, (h + 1) * sg)
            attended = jnp.where(
                lane_head == h, gathered[part] + own_weight[part] * value_new[mine], attended
            )
        attended = attended.astype(BF16)
        if g == 0:
            loads[3].wait()

        def outward(c):
            return jnp.concatenate(
                [
                    matmul(
                        attended,
                        wo[:, pl.ds(pl.multiple_of((2 * t + c) * slice_w, slice_w), slice_w)],
                    )
                    for t in range(levels)
                ],
                axis=1,
            )

        pair_send[g] = outward(1 - core).astype(BF16)
        remote(
            pair_send.at[g], pair_recv.at[g], pair_ss, pair_rs.at[g], {"tp": tp_at(1)}
        ).start()
        own_part[g] = outward(core)
    finish_pair(SEQ_GROUPS - 1)

    stream_half = jnp.concatenate(
        [
            stream[:, pl.ds(pl.multiple_of((2 * t + core) * slice_w, slice_w), slice_w)]
            for t in range(levels)
        ],
        axis=1,
    ).astype(F32)

    def transposed(src, dst):
        @pl.loop(0, n_tp)
        def _(t):
            into = lax.rem(t, 2) * half_w + lax.div(t, 2) * slice_w
            dst[pl.ds(pl.multiple_of(into, slice_w), slice_w), :] = src[
                :, pl.ds(pl.multiple_of(t * slice_w, slice_w), slice_w)
            ].T

    for g in range(SEQ_GROUPS):
        if g < 2:
            loads[4 + g].wait()
            transposed(*((wg, wg_t), (wu, wu_t))[g])
        total = stream_half[g * sg : (g + 1) * sg] + zs_send[g].astype(F32)
        wait_all(zs_recv.at[g, pl.ds(1, levels - 1)], zs_rs.at[g])
        for d in range(1, levels):
            total = total + zs_recv[g, d].astype(F32)
        mix[core, my_ep, g] = total.astype(BF16)
        here = mix.at[core, my_ep, g]
        for k in reversed(range(n_ep)):
            for c in range(2):
                if k or c:
                    remote(
                        here,
                        here,
                        mix_ss.at[c],
                        mix_rs.at[c],
                        {"ep": ep_at(k), "tp": tp_at(c)},
                    ).start()

    share = jnp.sum(
        jnp.where(routes[...] == my_ep, route_weights[...], 0.0), axis=0, keepdims=True
    )
    square = (tokens, tokens)
    diagonal = lax.broadcasted_iota(jnp.int32, square, 0) == lax.broadcasted_iota(
        jnp.int32, square, 1
    )
    coefficient = jnp.sum(jnp.where(diagonal, share, 0.0), axis=1, keepdims=True)
    loads[6].wait()
    wait_all(mix.at[0, others], mix_rs.at[0])
    wait_all(mix.at[1], mix_rs.at[1])
    halves = [mix[c].astype(F32).reshape(tokens, half_w) for c in range(2)]
    squares = sum(jnp.sum(half * half, axis=1, keepdims=True) for half in halves)
    inverse = lax.rsqrt(squares / width + 1e-06)
    normed_ffn = jnp.concatenate(
        [
            (
                halves[c]
                * inverse
                * jnp.concatenate(
                    [
                        gain_ffn[:, (2 * t + c) * slice_w : (2 * t + c + 1) * slice_w]
                        for t in range(levels)
                    ],
                    axis=1,
                )
            ).astype(BF16)
            for c in range(2)
        ],
        axis=1,
    )
    gate = matmul(normed_ffn, wg_t[...])
    up = matmul(normed_ffn, wu_t[...])
    hidden = (gate / (1.0 + jnp.exp(-gate)) * up).astype(BF16)

    def downward(c, d):
        at = (2 * flip(level, d) + c) * slice_w
        return matmul(hidden, wd[:, pl.ds(pl.multiple_of(at, slice_w), slice_w)]) * coefficient

    for d in reversed(range(levels)):
        dpair_send[d] = downward(1 - core, d).astype(BF16)
        remote(
            dpair_send.at[d], dpair_recv.at[d], dpair_ss, dpair_rs.at[d], {"tp": tp_at(1)}
        ).start()
    for d in range(levels):
        down_part[d] = downward(core, d)
    for d in reversed(range(levels)):
        wait_all(dpair_recv.at[d], dpair_rs.at[d])
        summed = down_part[d] + dpair_recv[d].astype(F32)
        for e in range(n_ep):
            fs_send[d, e] = summed[e * seqs : (e + 1) * seqs].astype(BF16)
        near = min(1, d)
        for k in reversed(range(n_ep)):
            if d or k:
                remote(
                    fs_send.at[d, ep_at(k)],
                    fs_recv.at[d, k],
                    fs_ss.at[near],
                    fs_rs.at[near],
                    {"ep": ep_at(k), "tp": tp_at(2 * d)},
                ).start()
    own_stream = mix[
        core, my_ep, :, :, pl.ds(pl.multiple_of(level * slice_w, slice_w), slice_w)
    ].astype(F32).reshape(seqs, slice_w)
    combined = own_stream + fs_send[0, my_ep].astype(F32)
    far = pl.ds(1, levels - 1)
    wait_all(fs_recv.at[far], fs_rs.at[1])
    wait_all(fs_recv.at[0, others], fs_rs.at[0])
    for d in range(levels):
        for k in range(n_ep):
            if d or k:
                combined = combined + fs_recv[d, k].astype(F32)
    out[...] = combined.astype(BF16)
    wait_all(a2a_send.at[others], a2a_ss)
    wait_all(part_recv.at[:, others], part_ss)
    wait_all(pair_send, pair_ss)
    wait_all(zs_recv.at[:, far], zs_ss)
    wait_all(mix.at[0, others], mix_ss.at[0])
    wait_all(mix.at[1], mix_ss.at[1])
    wait_all(dpair_send, dpair_ss)
    wait_all(fs_recv.at[far], fs_ss.at[1])
    wait_all(fs_recv.at[0, others], fs_ss.at[0])


def shards(
    stream,
    norm_gain_attn,
    w_query,
    w_key,
    w_value,
    w_forget,
    forget_bias,
    key_cache,
    value_cache,
    gate_cache,
    lengths,
    w_output,
    norm_gain_ffn,
    routes,
    route_weights,
    w_expert_gate,
    w_expert_up,
    expert_down_weight,
):
    n_ep = lax.axis_size("ep")
    n_tp = lax.axis_size("tp")
    seqs, width = stream.shape
    heads = gate_cache.shape[1]
    cache = key_cache.shape[1]
    depth, cols = w_query.shape
    hidden = w_expert_gate.shape[2]
    padded = -(-hidden // LANES) * LANES
    slice_w = width // n_tp
    levels = n_tp // 2
    half_w = levels * slice_w
    rows = heads * seqs
    sg = seqs // SEQ_GROUPS
    vmem = pl.BlockSpec(memory_space=pltpu.VMEM)
    hbm = pl.BlockSpec(memory_space=pltpu.HBM)
    dma = pltpu.SemaphoreType.DMA
    small = (
        stream,
        norm_gain_attn[None, :],
        w_forget.T,
        forget_bias[None, :],
        gate_cache,
        lengths[None, :],
        norm_gain_ffn[None, :],
        routes.T,
        route_weights.T,
    )
    return pl.pallas_call(
        functools.partial(layer_kernel, n_ep, n_tp, heads),
        out_shape=jax.ShapeDtypeStruct((seqs, slice_w), BF16),
        in_specs=[hbm] * 18,
        out_specs=vmem,
        scratch_shapes=[pltpu.VMEM(array.shape, array.dtype) for array in small]
        + [
            pltpu.VMEM((3, depth, cols), BF16),
            pltpu.VMEM((seqs, cache, cols), BF16),
            pltpu.VMEM((seqs * cols, cache), BF16),
            pltpu.VMEM((seqs, cache, cols), BF16),
            pltpu.VMEM((cols, width), BF16),
            pltpu.VMEM((padded, width), BF16),
            pltpu.VMEM((padded, width), BF16),
            pltpu.VMEM((padded, width), BF16),
            pltpu.VMEM((width, padded), BF16),
            pltpu.VMEM((width, padded), BF16),
            pltpu.VMEM((n_ep, seqs, depth), BF16),
            pltpu.VMEM((n_ep, seqs, depth), BF16),
            pltpu.VMEM((3, n_ep, seqs, cols), F32),
            pltpu.VMEM((3, n_ep, seqs, cols), F32),
            pltpu.VMEM((rows, cache), F32),
            pltpu.VMEM((SEQ_GROUPS, sg, half_w), BF16),
            pltpu.VMEM((SEQ_GROUPS, sg, half_w), BF16),
            pltpu.VMEM((SEQ_GROUPS, sg, half_w), F32),
            pltpu.VMEM((SEQ_GROUPS, sg, half_w), BF16),
            pltpu.VMEM((SEQ_GROUPS, levels, sg, half_w), BF16),
            pltpu.VMEM((2, n_ep, SEQ_GROUPS, sg, half_w), BF16),
            pltpu.VMEM((levels, n_ep * seqs, slice_w), BF16),
            pltpu.VMEM((levels, n_ep * seqs, slice_w), BF16),
            pltpu.VMEM((levels, n_ep * seqs, slice_w), F32),
            pltpu.VMEM((levels, n_ep, seqs, slice_w), BF16),
            pltpu.VMEM((levels, n_ep, seqs, slice_w), BF16),
            dma((len(small),)),
            dma((7,)),
            dma((CACHE_LOADS,)),
            dma((CACHE_LOADS,)),
            pltpu.SemaphoreType.REGULAR((max(1, levels.bit_length() - 2),)),
            dma,
            dma,
            dma,
            dma((3,)),
            dma,
            dma((SEQ_GROUPS,)),
            dma,
            dma((SEQ_GROUPS,)),
            dma((2,)),
            dma((2,)),
            dma,
            dma((levels,)),
            dma((2,)),
            dma((2,)),
        ],
        compiler_params=pltpu.CompilerParams(
            collective_id=0, has_side_effects=True, vmem_limit_bytes=48 * 1024 * 1024
        ),
    )(
        *(
            pltpu.with_memory_space_constraint(array, pltpu.HBM)
            for array in (
                *small,
                w_query,
                w_key,
                w_value,
                key_cache,
                value_cache,
                w_output,
                jnp.swapaxes(w_expert_gate, 1, 2),
                jnp.swapaxes(w_expert_up, 1, 2),
                expert_down_weight,
            )
        )
    )


def solution(mesh):
    placed = (
        P("ep", None),
        P(),
        P("ep", "tp"),
        P("ep", "tp"),
        P("ep", "tp"),
        P(),
        P(),
        P("ep", None, "tp"),
        P("ep", None, "tp"),
        P("ep", "tp", None),
        P("ep"),
        P("tp", None),
        P(),
        P(),
        P(),
        P("ep", None, "tp"),
        P("ep", None, "tp"),
        P("ep", "tp", None),
    )
    return jax.shard_map(
        shards, mesh=mesh, in_specs=placed, out_specs=P("ep", "tp"), check_vma=False
    )
```

```python
import functools

import jax
import jax.numpy as jnp
from jax import lax
from jax.experimental import pallas as pl
from jax.experimental.pallas import tpu as pltpu
from jax.sharding import PartitionSpec as P

F32 = jnp.float32
BF16 = jnp.bfloat16
SEQ_GROUPS = 2
CACHE_LOADS = 4
LANES = 128


def inverse_rms(floats):
    return lax.rsqrt(jnp.mean(floats * floats, axis=-1, keepdims=True) + 1e-06)


def matmul(a, b):
    return jnp.dot(a, b, preferred_element_type=F32)


def matmul_t(a, b):
    return lax.dot_general(a, b, (((1,), (1,)), ((), ())), preferred_element_type=F32)


def flip(index, bits):
    moved, bit = index, 1
    while bit <= bits:
        if bits & bit:
            moved = moved + bit - 2 * bit * lax.rem(lax.div(index, bit), 2)
        bit *= 2
    return moved


def layer_kernel(
    n_ep,
    n_tp,
    heads,
    stream_hbm,
    gain_attn_hbm,
    w_forget_hbm,
    forget_bias_hbm,
    gates_hbm,
    lengths_hbm,
    gain_ffn_hbm,
    routes_hbm,
    route_weights_hbm,
    wq_hbm,
    wk_hbm,
    wv_hbm,
    keys_hbm,
    values_hbm,
    wo_hbm,
    wg_hbm,
    wu_hbm,
    wd_hbm,
    out,
    stream,
    gain_attn,
    w_forget,
    forget_bias,
    gates,
    lengths,
    gain_ffn,
    routes,
    route_weights,
    wqkv,
    keys,
    keys_t,
    values,
    wo,
    wg,
    wu,
    wd,
    wg_t,
    wu_t,
    a2a_send,
    a2a_recv,
    part_send,
    part_recv,
    gate_rows,
    pair_send,
    pair_recv,
    own_part,
    zs_send,
    zs_recv,
    zfar_send,
    zfar_recv,
    mix,
    dpair_send,
    dpair_recv,
    down_part,
    fs_send,
    fs_recv,
    small_sem,
    w_sem,
    k_sem,
    v_sem,
    relay,
    a2a_ss,
    a2a_rs,
    part_ss,
    part_rs,
    pair_ss,
    pair_rs,
    zs_ss,
    zs_rs,
    zfar_ss,
    zfar_rs,
    mix_ss,
    mix_rs,
    dpair_ss,
    dpair_rs,
    fs_ss,
    fs_rs,
):
    my_ep = lax.axis_index("ep")
    my_tp = lax.axis_index("tp")
    seqs, width = stream.shape
    depth = wq_hbm.shape[0]
    cols = wq_hbm.shape[1]
    cache = keys.shape[1]
    head_dim = cols // heads
    slice_w = out.shape[1]
    hidden_w = wg_hbm.shape[1]
    tokens = n_ep * seqs
    levels = n_tp // 2
    half_w = levels * slice_w
    core, level = lax.rem(my_tp, 2), lax.div(my_tp, 2)
    sg = seqs // SEQ_GROUPS
    grows = heads * sg
    rows = SEQ_GROUPS * grows

    def ep_at(k):
        return flip(my_ep, k)

    def tp_at(d):
        return flip(my_tp, d)

    def remote(src, dst, ss, rs, device):
        return pltpu.make_async_remote_copy(
            src_ref=src,
            dst_ref=dst,
            send_sem=ss,
            recv_sem=rs,
            device_id=device,
            device_id_type=pl.DeviceIdType.MESH,
        )

    def wait_all(ref, sem):
        pltpu.make_async_copy(ref, ref, sem).wait()

    others = pl.ds(1, n_ep - 1)
    barrier = pltpu.get_barrier_semaphore()
    bits = [1 << b for b in range(levels.bit_length() - 1)]
    met = [{"ep": ep_at(k)} for k in reversed(range(1, n_ep))]
    met += [{"tp": tp_at(1)}] + [{"tp": tp_at(2 * b)} for b in bits]
    for device in met:
        pl.semaphore_signal(barrier, inc=1, device_id=device, device_id_type=pl.DeviceIdType.MESH)

    small = [
        pltpu.make_async_copy(src, dst, small_sem.at[i])
        for i, (src, dst) in enumerate(
            (
                (stream_hbm, stream),
                (gain_attn_hbm, gain_attn),
                (w_forget_hbm, w_forget),
                (forget_bias_hbm, forget_bias),
                (gates_hbm, gates),
                (lengths_hbm, lengths),
                (gain_ffn_hbm, gain_ffn),
                (routes_hbm, routes),
                (route_weights_hbm, route_weights),
            )
        )
    ]
    loads = [
        pltpu.make_async_copy(src, dst, w_sem.at[i])
        for i, (src, dst) in enumerate(
            (
                (wq_hbm, wqkv.at[0]),
                (wk_hbm, wqkv.at[1]),
                (wv_hbm, wqkv.at[2]),
                (wo_hbm, wo),
                (wg_hbm.at[0], wg.at[pl.ds(0, hidden_w)]),
                (wu_hbm.at[0], wu.at[pl.ds(0, hidden_w)]),
                (wd_hbm.at[0], wd.at[pl.ds(0, hidden_w)]),
            )
        )
    ]
    span = seqs // CACHE_LOADS
    key_loads = [
        pltpu.make_async_copy(
            keys_hbm.at[pl.ds(i * span, span)], keys.at[pl.ds(i * span, span)], k_sem.at[i]
        )
        for i in range(CACHE_LOADS)
    ]
    value_loads = [
        pltpu.make_async_copy(
            values_hbm.at[pl.ds(i * span, span)], values.at[pl.ds(i * span, span)], v_sem.at[i]
        )
        for i in range(CACHE_LOADS)
    ]
    for load in small[:2] + loads[:3] + small[2:]:
        load.start()
    for load in key_loads:
        load.start(priority=1)

    spare = wg.shape[0] - hidden_w
    if spare:
        for w in (wg, wu, wd):
            w[hidden_w:, :] = jnp.zeros((spare, width), BF16)

    small[0].wait()
    small[1].wait()
    floats = stream[...].astype(F32)
    normed = (floats * inverse_rms(floats) * gain_attn[...]).astype(BF16)
    for e in range(n_ep):
        a2a_send[e] = normed[:, e * depth : (e + 1) * depth]

    pl.semaphore_wait(barrier, len(met))

    for k in reversed(range(1, n_ep)):
        remote(a2a_send.at[ep_at(k)], a2a_recv.at[k], a2a_ss, a2a_rs, {"ep": ep_at(k)}).start()
    a2a_recv[0] = a2a_send[my_ep]
    for load in value_loads:
        load.start(priority=1)
    for i, b in enumerate(bits[:-1]):
        pl.semaphore_signal(
            relay.at[i],
            inc=1,
            device_id={"tp": tp_at(2 * b)},
            device_id_type=pl.DeviceIdType.MESH,
        )
        pl.semaphore_wait(relay.at[i], 1)
    pl.semaphore_signal(
        relay.at[len(bits) - 1],
        inc=1,
        device_id={"tp": tp_at(1)},
        device_id_type=pl.DeviceIdType.MESH,
    )
    pl.semaphore_wait(relay.at[len(bits) - 1], 1)

    for load in small[2:]:
        load.wait()
    forget_all = matmul_t(normed, w_forget[...]) + forget_bias[...]
    forget_all = -(jnp.maximum(-forget_all, 0.0) + jnp.log1p(jnp.exp(-jnp.abs(forget_all))))
    head_lane = lax.broadcasted_iota(jnp.int32, (sg, forget_all.shape[1]), 1)
    forget_new = jnp.concatenate(
        [
            jnp.sum(
                jnp.where(
                    head_lane == my_tp * heads + h, forget_all[g * sg : (g + 1) * sg], 0.0
                ),
                axis=1,
                keepdims=True,
            )
            for g in range(SEQ_GROUPS)
            for h in range(heads)
        ],
        axis=0,
    )
    for g in range(SEQ_GROUPS):
        for h in range(heads):
            for s in range(sg):
                r = (g * heads + h) * sg + s
                gate_rows[r : r + 1, :] = gates[g * sg + s, h : h + 1, :]
    row = lax.broadcasted_iota(jnp.int32, (rows, seqs), 0)
    row_seq = row // grows * sg + row % sg
    length_f = lengths[...].astype(F32)
    live_count = jnp.sum(
        jnp.where(lax.broadcasted_iota(jnp.int32, (rows, seqs), 1) == row_seq, length_f, 0.0),
        axis=1,
        keepdims=True,
    ).astype(jnp.int32)
    position = lax.broadcasted_iota(jnp.int32, (rows, cache), 1)
    last_gate = jnp.sum(
        jnp.where(position == live_count - 1, gate_rows[...], 0.0), axis=1, keepdims=True
    )
    gate_rows[...] = jnp.where(
        position < live_count, forget_new + (last_gate - gate_rows[...]), -1e30
    )

    for i in range(CACHE_LOADS // 2):
        key_loads[i].wait()

        @pl.loop(i * span, (i + 1) * span)
        def _(s):
            keys_t[pl.ds(pl.multiple_of(s * cols, cols), cols), :] = keys[s].T

    for load in loads[:3]:
        load.wait()
    wait_all(a2a_recv.at[others], a2a_rs)
    block = a2a_recv[...].reshape(tokens, depth)
    for i in range(3):
        product = matmul(block, wqkv[i])
        for k in reversed(range(1, n_ep)):
            part_send[i, k] = product[k * seqs : (k + 1) * seqs]
            remote(
                part_send.at[i, k], part_recv.at[i, k], part_ss, part_rs.at[i], {"ep": ep_at(k)}
            ).start()
        part_recv[i, 0] = product[:seqs]

    for load in loads[3:]:
        load.start(priority=1)

    for i in range(CACHE_LOADS // 2, CACHE_LOADS):
        key_loads[i].wait()

        @pl.loop(i * span, (i + 1) * span)
        def _(s):
            keys_t[pl.ds(pl.multiple_of(s * cols, cols), cols), :] = keys[s].T

    def projected(i):
        wait_all(part_recv.at[i, others], part_rs.at[i])
        total = part_recv[i, 0]
        for e in range(1, n_ep):
            total = total + part_recv[i, e]
        return total.astype(BF16).astype(F32)

    scale = head_dim ** (-0.5)
    query = projected(0)
    lane_head = lax.broadcasted_iota(jnp.int32, (sg, cols), 1) // head_dim
    group_seq = lax.broadcasted_iota(jnp.int32, (grows, 1), 0) % sg

    def by_head(values_of):
        return jnp.concatenate(values_of, axis=0)

    def score(g):
        mine = query[g * sg : (g + 1) * sg]
        spread = by_head([jnp.where(lane_head == h, mine, 0.0) for h in range(heads)])
        lhs = jnp.concatenate(
            [jnp.where(group_seq == s, spread, 0.0).astype(BF16) for s in range(sg)], axis=1
        )
        return matmul(lhs, keys_t[g * sg * cols : (g + 1) * sg * cols, :])

    def finish_pair(g):
        wait_all(pair_recv.at[g], pair_rs.at[g])
        zs_send[g] = (own_part[g] + pair_recv[g].astype(F32)).astype(BF16)
        for d in reversed(range(1, levels - 1)):
            remote(
                zs_send.at[g], zs_recv.at[g, d], zs_ss, zs_rs.at[g], {"tp": tp_at(2 * d)}
            ).start()

    def soften(g, found):
        mine = slice(g * sg, (g + 1) * sg)
        own_score = (
            by_head(
                [
                    jnp.sum(
                        jnp.where(lane_head == h, query[mine] * key_new[mine], 0.0),
                        axis=1,
                        keepdims=True,
                    )
                    for h in range(heads)
                ]
            )
            * scale
        )
        full = found * scale + gate_rows[g * grows : (g + 1) * grows, :]
        largest = jnp.maximum(jnp.max(full, axis=1, keepdims=True), own_score)
        past = jnp.exp(full - largest)
        own_term = jnp.exp(own_score - largest)
        total = jnp.sum(past, axis=1, keepdims=True) + own_term
        return past / total, (own_term / total).astype(BF16).astype(F32)

    found = score(0)
    key_new = projected(1)
    value_new = projected(2)
    for load in value_loads:
        load.wait()
    loads[3].wait()
    softened = []
    for g in range(SEQ_GROUPS):
        later = score(g + 1) if g + 1 < SEQ_GROUPS else None
        softened.append(soften(g, found))
        found = later
    for g in range(SEQ_GROUPS):
        mine = slice(g * sg, (g + 1) * sg)
        past_weights, own_weight = softened[g]
        gathered = jnp.zeros((grows, cols), F32)
        for s in range(sg):
            chosen = jnp.where(group_seq == s, past_weights, 0.0).astype(BF16)
            gathered = gathered + matmul(chosen, values[g * sg + s])
        attended = jnp.zeros((sg, cols), F32)
        for h in range(heads):
            part = slice(h * sg, (h + 1) * sg)
            attended = jnp.where(
                lane_head == h, gathered[part] + own_weight[part] * value_new[mine], attended
            )
        attended = attended.astype(BF16)
        if g:
            finish_pair(g - 1)

        def outward(c):
            return jnp.concatenate(
                [
                    matmul(
                        attended,
                        wo[:, pl.ds(pl.multiple_of((2 * t + c) * slice_w, slice_w), slice_w)],
                    )
                    for t in range(levels)
                ],
                axis=1,
            )

        pair_send[g] = outward(1 - core).astype(BF16)
        last = 2 * (levels - 1)
        remote(
            pair_send.at[g], zfar_recv.at[g, 1], zfar_ss, zfar_rs.at[g], {"tp": tp_at(last + 1)}
        ).start()
        remote(
            pair_send.at[g], pair_recv.at[g], pair_ss, pair_rs.at[g], {"tp": tp_at(1)}
        ).start()
        own_part[g] = outward(core)
        zfar_send[g] = own_part[g].astype(BF16)
        remote(
            zfar_send.at[g], zfar_recv.at[g, 0], zfar_ss, zfar_rs.at[g], {"tp": tp_at(last)}
        ).start()
    def transposed(src, dst, low, high):
        @pl.loop(low, high)
        def _(t):
            into = lax.rem(t, 2) * half_w + lax.div(t, 2) * slice_w
            dst[pl.ds(pl.multiple_of(into, slice_w), slice_w), :] = src[
                :, pl.ds(pl.multiple_of(t * slice_w, slice_w), slice_w)
            ].T

    loads[4].wait()
    loads[5].wait()
    transposed(wg, wg_t, 0, n_tp // 2)
    finish_pair(SEQ_GROUPS - 1)
    transposed(wg, wg_t, n_tp // 2, n_tp)
    transposed(wu, wu_t, 0, n_tp)

    stream_half = jnp.concatenate(
        [
            stream[:, pl.ds(pl.multiple_of((2 * t + core) * slice_w, slice_w), slice_w)]
            for t in range(levels)
        ],
        axis=1,
    ).astype(F32)

    for g in range(SEQ_GROUPS):
        total = stream_half[g * sg : (g + 1) * sg] + zs_send[g].astype(F32)
        wait_all(zs_recv.at[g, pl.ds(1, levels - 2)], zs_rs.at[g])
        for d in range(1, levels - 1):
            total = total + zs_recv[g, d].astype(F32)
        wait_all(zfar_recv.at[g], zfar_rs.at[g])
        total = total + zfar_recv[g, 0].astype(F32) + zfar_recv[g, 1].astype(F32)
        mix[core, my_ep, g] = total.astype(BF16)
        here = mix.at[core, my_ep, g]
        for k in reversed(range(n_ep)):
            for c in range(2):
                if k or c:
                    remote(
                        here,
                        here,
                        mix_ss.at[c],
                        mix_rs.at[c],
                        {"ep": ep_at(k), "tp": tp_at(c)},
                    ).start()

    share = jnp.sum(
        jnp.where(routes[...] == my_ep, route_weights[...], 0.0), axis=0, keepdims=True
    )
    square = (tokens, tokens)
    diagonal = lax.broadcasted_iota(jnp.int32, square, 0) == lax.broadcasted_iota(
        jnp.int32, square, 1
    )
    coefficient = jnp.sum(jnp.where(diagonal, share, 0.0), axis=1, keepdims=True)
    loads[6].wait()
    wait_all(mix.at[0, others], mix_rs.at[0])
    wait_all(mix.at[1], mix_rs.at[1])
    halves = [mix[c].astype(F32).reshape(tokens, half_w) for c in range(2)]
    squares = sum(jnp.sum(half * half, axis=1, keepdims=True) for half in halves)
    inverse = lax.rsqrt(squares / width + 1e-06)
    normed_ffn = jnp.concatenate(
        [
            (
                halves[c]
                * inverse
                * jnp.concatenate(
                    [
                        gain_ffn[:, (2 * t + c) * slice_w : (2 * t + c + 1) * slice_w]
                        for t in range(levels)
                    ],
                    axis=1,
                )
            ).astype(BF16)
            for c in range(2)
        ],
        axis=1,
    )
    gate = matmul(normed_ffn, wg_t[...])
    up = matmul(normed_ffn, wu_t[...])
    hidden = (gate / (1.0 + jnp.exp(-gate)) * up).astype(BF16)

    def downward(c, d):
        at = (2 * flip(level, d) + c) * slice_w
        return matmul(hidden, wd[:, pl.ds(pl.multiple_of(at, slice_w), slice_w)]) * coefficient

    for d in reversed(range(levels)):
        dpair_send[d] = downward(1 - core, d).astype(BF16)
        remote(
            dpair_send.at[d], dpair_recv.at[d], dpair_ss, dpair_rs.at[d], {"tp": tp_at(1)}
        ).start()
    for d in range(levels):
        down_part[d] = downward(core, d)
    for d in reversed(range(levels)):
        wait_all(dpair_recv.at[d], dpair_rs.at[d])
        summed = down_part[d] + dpair_recv[d].astype(F32)
        for e in range(n_ep):
            fs_send[d, e] = summed[e * seqs : (e + 1) * seqs].astype(BF16)
        near = min(1, d)
        for k in reversed(range(n_ep)):
            if d or k:
                remote(
                    fs_send.at[d, ep_at(k)],
                    fs_recv.at[d, k],
                    fs_ss.at[near],
                    fs_rs.at[near],
                    {"ep": ep_at(k), "tp": tp_at(2 * d)},
                ).start()
    own_stream = mix[
        core, my_ep, :, :, pl.ds(pl.multiple_of(level * slice_w, slice_w), slice_w)
    ].astype(F32).reshape(seqs, slice_w)
    combined = own_stream + fs_send[0, my_ep].astype(F32)
    far = pl.ds(1, levels - 1)
    wait_all(fs_recv.at[far], fs_rs.at[1])
    wait_all(fs_recv.at[0, others], fs_rs.at[0])
    for d in range(levels):
        for k in range(n_ep):
            if d or k:
                combined = combined + fs_recv[d, k].astype(F32)
    out[...] = combined.astype(BF16)
    wait_all(a2a_send.at[others], a2a_ss)
    wait_all(part_recv.at[:, others], part_ss)
    wait_all(pair_send, pair_ss)
    wait_all(zs_recv.at[:, pl.ds(1, levels - 2)], zs_ss)
    wait_all(zfar_recv, zfar_ss)
    wait_all(mix.at[0, others], mix_ss.at[0])
    wait_all(mix.at[1], mix_ss.at[1])
    wait_all(dpair_send, dpair_ss)
    wait_all(fs_recv.at[far], fs_ss.at[1])
    wait_all(fs_recv.at[0, others], fs_ss.at[0])


def shards(
    stream,
    norm_gain_attn,
    w_query,
    w_key,
    w_value,
    w_forget,
    forget_bias,
    key_cache,
    value_cache,
    gate_cache,
    lengths,
    w_output,
    norm_gain_ffn,
    routes,
    route_weights,
    w_expert_gate,
    w_expert_up,
    expert_down_weight,
):
    n_ep = lax.axis_size("ep")
    n_tp = lax.axis_size("tp")
    seqs, width = stream.shape
    heads = gate_cache.shape[1]
    cache = key_cache.shape[1]
    depth, cols = w_query.shape
    hidden = w_expert_gate.shape[2]
    padded = -(-hidden // LANES) * LANES
    slice_w = width // n_tp
    levels = n_tp // 2
    half_w = levels * slice_w
    rows = heads * seqs
    sg = seqs // SEQ_GROUPS
    vmem = pl.BlockSpec(memory_space=pltpu.VMEM)
    hbm = pl.BlockSpec(memory_space=pltpu.HBM)
    dma = pltpu.SemaphoreType.DMA
    small = (
        stream,
        norm_gain_attn[None, :],
        w_forget.T,
        forget_bias[None, :],
        gate_cache,
        lengths[None, :],
        norm_gain_ffn[None, :],
        routes.T,
        route_weights.T,
    )
    return pl.pallas_call(
        functools.partial(layer_kernel, n_ep, n_tp, heads),
        out_shape=jax.ShapeDtypeStruct((seqs, slice_w), BF16),
        in_specs=[hbm] * 18,
        out_specs=vmem,
        scratch_shapes=[pltpu.VMEM(array.shape, array.dtype) for array in small]
        + [
            pltpu.VMEM((3, depth, cols), BF16),
            pltpu.VMEM((seqs, cache, cols), BF16),
            pltpu.VMEM((seqs * cols, cache), BF16),
            pltpu.VMEM((seqs, cache, cols), BF16),
            pltpu.VMEM((cols, width), BF16),
            pltpu.VMEM((padded, width), BF16),
            pltpu.VMEM((padded, width), BF16),
            pltpu.VMEM((padded, width), BF16),
            pltpu.VMEM((width, padded), BF16),
            pltpu.VMEM((width, padded), BF16),
            pltpu.VMEM((n_ep, seqs, depth), BF16),
            pltpu.VMEM((n_ep, seqs, depth), BF16),
            pltpu.VMEM((3, n_ep, seqs, cols), F32),
            pltpu.VMEM((3, n_ep, seqs, cols), F32),
            pltpu.VMEM((rows, cache), F32),
            pltpu.VMEM((SEQ_GROUPS, sg, half_w), BF16),
            pltpu.VMEM((SEQ_GROUPS, sg, half_w), BF16),
            pltpu.VMEM((SEQ_GROUPS, sg, half_w), F32),
            pltpu.VMEM((SEQ_GROUPS, sg, half_w), BF16),
            pltpu.VMEM((SEQ_GROUPS, levels, sg, half_w), BF16),
            pltpu.VMEM((SEQ_GROUPS, sg, half_w), BF16),
            pltpu.VMEM((SEQ_GROUPS, 2, sg, half_w), BF16),
            pltpu.VMEM((2, n_ep, SEQ_GROUPS, sg, half_w), BF16),
            pltpu.VMEM((levels, n_ep * seqs, slice_w), BF16),
            pltpu.VMEM((levels, n_ep * seqs, slice_w), BF16),
            pltpu.VMEM((levels, n_ep * seqs, slice_w), F32),
            pltpu.VMEM((levels, n_ep, seqs, slice_w), BF16),
            pltpu.VMEM((levels, n_ep, seqs, slice_w), BF16),
            dma((len(small),)),
            dma((7,)),
            dma((CACHE_LOADS,)),
            dma((CACHE_LOADS,)),
            pltpu.SemaphoreType.REGULAR((levels.bit_length() - 1,)),
            dma,
            dma,
            dma,
            dma((3,)),
            dma,
            dma((SEQ_GROUPS,)),
            dma,
            dma((SEQ_GROUPS,)),
            dma,
            dma((SEQ_GROUPS,)),
            dma((2,)),
            dma((2,)),
            dma,
            dma((levels,)),
            dma((2,)),
            dma((2,)),
        ],
        compiler_params=pltpu.CompilerParams(
            collective_id=0, has_side_effects=True, vmem_limit_bytes=48 * 1024 * 1024
        ),
    )(
        *(
            pltpu.with_memory_space_constraint(array, pltpu.HBM)
            for array in (
                *small,
                w_query,
                w_key,
                w_value,
                key_cache,
                value_cache,
                w_output,
                jnp.swapaxes(w_expert_gate, 1, 2),
                jnp.swapaxes(w_expert_up, 1, 2),
                expert_down_weight,
            )
        )
    )


def solution(mesh):
    placed = (
        P("ep", None),
        P(),
        P("ep", "tp"),
        P("ep", "tp"),
        P("ep", "tp"),
        P(),
        P(),
        P("ep", None, "tp"),
        P("ep", None, "tp"),
        P("ep", "tp", None),
        P("ep"),
        P("tp", None),
        P(),
        P(),
        P(),
        P("ep", None, "tp"),
        P("ep", None, "tp"),
        P("ep", "tp", None),
    )
    return jax.shard_map(
        shards, mesh=mesh, in_specs=placed, out_specs=P("ep", "tp"), check_vma=False
    )
```

```python
import functools

import jax
import jax.numpy as jnp
from jax import lax
from jax.experimental import pallas as pl
from jax.experimental.pallas import tpu as pltpu
from jax.sharding import PartitionSpec as P

F32 = jnp.float32
BF16 = jnp.bfloat16
SEQ_GROUPS = 2
CACHE_LOADS = 4
LANES = 128


def inverse_rms(floats):
    return lax.rsqrt(jnp.mean(floats * floats, axis=-1, keepdims=True) + 1e-06)


def matmul(a, b):
    return jnp.dot(a, b, preferred_element_type=F32)


def matmul_t(a, b):
    return lax.dot_general(a, b, (((1,), (1,)), ((), ())), preferred_element_type=F32)


def flip(index, bits):
    moved, bit = index, 1
    while bit <= bits:
        if bits & bit:
            moved = moved + bit - 2 * bit * lax.rem(lax.div(index, bit), 2)
        bit *= 2
    return moved


def layer_kernel(
    n_ep,
    n_tp,
    heads,
    stream_hbm,
    gain_attn_hbm,
    w_forget_hbm,
    forget_bias_hbm,
    gates_hbm,
    lengths_hbm,
    gain_ffn_hbm,
    routes_hbm,
    route_weights_hbm,
    wq_hbm,
    wk_hbm,
    wv_hbm,
    keys_hbm,
    values_hbm,
    wo_hbm,
    wg_hbm,
    wu_hbm,
    wd_hbm,
    out,
    stream,
    gain_attn,
    w_forget,
    forget_bias,
    gates,
    lengths,
    gain_ffn,
    routes,
    route_weights,
    wqkv,
    keys,
    keys_t,
    values,
    wo,
    wg,
    wu,
    wd,
    wg_t,
    wu_t,
    a2a_send,
    a2a_recv,
    part_send,
    part_recv,
    gate_rows,
    pair_send,
    pair_recv,
    own_part,
    zs_send,
    zs_recv,
    zfar_send,
    zfar_recv,
    mix,
    dpair_send,
    dpair_recv,
    down_part,
    fs_send,
    fs_recv,
    small_sem,
    w_sem,
    k_sem,
    v_sem,
    relay,
    a2a_ss,
    a2a_rs,
    part_ss,
    part_rs,
    pair_ss,
    pair_rs,
    zs_ss,
    zs_rs,
    zfar_ss,
    zfar_rs,
    mix_ss,
    mix_rs,
    dpair_ss,
    dpair_rs,
    fs_ss,
    fs_rs,
):
    my_ep = lax.axis_index("ep")
    my_tp = lax.axis_index("tp")
    seqs, width = stream.shape
    depth = wq_hbm.shape[0]
    cols = wq_hbm.shape[1]
    cache = keys.shape[1]
    head_dim = cols // heads
    slice_w = out.shape[1]
    hidden_w = wg_hbm.shape[1]
    tokens = n_ep * seqs
    levels = n_tp // 2
    half_w = levels * slice_w
    core, level = lax.rem(my_tp, 2), lax.div(my_tp, 2)
    sg = seqs // SEQ_GROUPS
    grows = heads * sg
    rows = SEQ_GROUPS * grows

    def ep_at(k):
        return flip(my_ep, k)

    def tp_at(d):
        return flip(my_tp, d)

    def remote(src, dst, ss, rs, device):
        return pltpu.make_async_remote_copy(
            src_ref=src,
            dst_ref=dst,
            send_sem=ss,
            recv_sem=rs,
            device_id=device,
            device_id_type=pl.DeviceIdType.MESH,
        )

    def wait_all(ref, sem):
        pltpu.make_async_copy(ref, ref, sem).wait()

    others = pl.ds(1, n_ep - 1)
    barrier = pltpu.get_barrier_semaphore()
    bits = [1 << b for b in range(levels.bit_length() - 1)]
    met = [{"ep": ep_at(k)} for k in reversed(range(1, n_ep))]
    met += [{"tp": tp_at(1)}] + [{"tp": tp_at(2 * b)} for b in bits]
    for device in met:
        pl.semaphore_signal(barrier, inc=1, device_id=device, device_id_type=pl.DeviceIdType.MESH)

    small = [
        pltpu.make_async_copy(src, dst, small_sem.at[i])
        for i, (src, dst) in enumerate(
            (
                (stream_hbm, stream),
                (gain_attn_hbm, gain_attn),
                (w_forget_hbm, w_forget),
                (forget_bias_hbm, forget_bias),
                (gates_hbm, gates),
                (lengths_hbm, lengths),
                (gain_ffn_hbm, gain_ffn),
                (routes_hbm, routes),
                (route_weights_hbm, route_weights),
            )
        )
    ]
    loads = [
        pltpu.make_async_copy(src, dst, w_sem.at[i])
        for i, (src, dst) in enumerate(
            (
                (wq_hbm, wqkv.at[0]),
                (wk_hbm, wqkv.at[1]),
                (wv_hbm, wqkv.at[2]),
                (wo_hbm, wo),
                (wg_hbm.at[0], wg.at[pl.ds(0, hidden_w)]),
                (wu_hbm.at[0], wu.at[pl.ds(0, hidden_w)]),
                (wd_hbm.at[0], wd.at[pl.ds(0, hidden_w)]),
            )
        )
    ]
    span = seqs // CACHE_LOADS
    key_loads = [
        pltpu.make_async_copy(
            keys_hbm.at[pl.ds(i * span, span)], keys.at[pl.ds(i * span, span)], k_sem.at[i]
        )
        for i in range(CACHE_LOADS)
    ]
    value_loads = [
        pltpu.make_async_copy(
            values_hbm.at[pl.ds(i * span, span)], values.at[pl.ds(i * span, span)], v_sem.at[i]
        )
        for i in range(CACHE_LOADS)
    ]
    for load in small[:2] + loads[:3] + small[2:]:
        load.start()
    for load in key_loads:
        load.start(priority=1)

    spare = wg.shape[0] - hidden_w
    if spare:
        for w in (wg, wu, wd):
            w[hidden_w:, :] = jnp.zeros((spare, width), BF16)

    small[0].wait()
    small[1].wait()
    floats = stream[...].astype(F32)
    normed = (floats * inverse_rms(floats) * gain_attn[...]).astype(BF16)
    for e in range(n_ep):
        a2a_send[e] = normed[:, e * depth : (e + 1) * depth]

    pl.semaphore_wait(barrier, len(met))

    for k in reversed(range(1, n_ep)):
        remote(a2a_send.at[ep_at(k)], a2a_recv.at[k], a2a_ss, a2a_rs, {"ep": ep_at(k)}).start()
    a2a_recv[0] = a2a_send[my_ep]
    for load in value_loads:
        load.start(priority=1)

    def tell(i, d):
        pl.semaphore_signal(
            relay.at[i],
            inc=1,
            device_id={"tp": tp_at(d)},
            device_id_type=pl.DeviceIdType.MESH,
        )

    tell(0, 2 * bits[0])

    for load in small[2:]:
        load.wait()
    forget_all = matmul_t(normed, w_forget[...]) + forget_bias[...]
    forget_all = -(jnp.maximum(-forget_all, 0.0) + jnp.log1p(jnp.exp(-jnp.abs(forget_all))))
    head_lane = lax.broadcasted_iota(jnp.int32, (sg, forget_all.shape[1]), 1)
    forget_new = jnp.concatenate(
        [
            jnp.sum(
                jnp.where(
                    head_lane == my_tp * heads + h, forget_all[g * sg : (g + 1) * sg], 0.0
                ),
                axis=1,
                keepdims=True,
            )
            for g in range(SEQ_GROUPS)
            for h in range(heads)
        ],
        axis=0,
    )
    for g in range(SEQ_GROUPS):
        for h in range(heads):
            for s in range(sg):
                r = (g * heads + h) * sg + s
                gate_rows[r : r + 1, :] = gates[g * sg + s, h : h + 1, :]
    row = lax.broadcasted_iota(jnp.int32, (rows, seqs), 0)
    row_seq = row // grows * sg + row % sg
    length_f = lengths[...].astype(F32)
    live_count = jnp.sum(
        jnp.where(lax.broadcasted_iota(jnp.int32, (rows, seqs), 1) == row_seq, length_f, 0.0),
        axis=1,
        keepdims=True,
    ).astype(jnp.int32)
    position = lax.broadcasted_iota(jnp.int32, (rows, cache), 1)
    last_gate = jnp.sum(
        jnp.where(position == live_count - 1, gate_rows[...], 0.0), axis=1, keepdims=True
    )
    gate_rows[...] = jnp.where(
        position < live_count, forget_new + (last_gate - gate_rows[...]), -1e30
    )

    for i in range(CACHE_LOADS // 2):
        key_loads[i].wait()

        @pl.loop(i * span, (i + 1) * span)
        def _(s):
            keys_t[pl.ds(pl.multiple_of(s * cols, cols), cols), :] = keys[s].T

    for load in loads[:3]:
        load.wait()
    wait_all(a2a_recv.at[others], a2a_rs)
    block = a2a_recv[...].reshape(tokens, depth)
    for i in range(3):
        product = matmul(block, wqkv[i])
        for k in reversed(range(1, n_ep)):
            part_send[i, k] = product[k * seqs : (k + 1) * seqs]
            remote(
                part_send.at[i, k], part_recv.at[i, k], part_ss, part_rs.at[i], {"ep": ep_at(k)}
            ).start()
        part_recv[i, 0] = product[:seqs]

    for load in loads[3:]:
        load.start(priority=1)

    for i in range(len(bits) - 1):
        pl.semaphore_wait(relay.at[i], 1)
        tell(i + 1, 2 * bits[i + 1] if i + 2 < len(bits) else 1)

    for i in range(CACHE_LOADS // 2, CACHE_LOADS):
        key_loads[i].wait()

        @pl.loop(i * span, (i + 1) * span)
        def _(s):
            keys_t[pl.ds(pl.multiple_of(s * cols, cols), cols), :] = keys[s].T

    def projected(i):
        wait_all(part_recv.at[i, others], part_rs.at[i])
        total = part_recv[i, 0]
        for e in range(1, n_ep):
            total = total + part_recv[i, e]
        return total.astype(BF16).astype(F32)

    scale = head_dim ** (-0.5)
    query = projected(0)
    lane_head = lax.broadcasted_iota(jnp.int32, (sg, cols), 1) // head_dim
    group_seq = lax.broadcasted_iota(jnp.int32, (grows, 1), 0) % sg

    def by_head(values_of):
        return jnp.concatenate(values_of, axis=0)

    def score(g):
        mine = query[g * sg : (g + 1) * sg]
        spread = by_head([jnp.where(lane_head == h, mine, 0.0) for h in range(heads)])
        lhs = jnp.concatenate(
            [jnp.where(group_seq == s, spread, 0.0).astype(BF16) for s in range(sg)], axis=1
        )
        return matmul(lhs, keys_t[g * sg * cols : (g + 1) * sg * cols, :])

    def finish_pair(g):
        wait_all(pair_recv.at[g], pair_rs.at[g])
        zs_send[g] = (own_part[g] + pair_recv[g].astype(F32)).astype(BF16)
        for d in reversed(range(1, levels - 1)):
            remote(
                zs_send.at[g], zs_recv.at[g, d], zs_ss, zs_rs.at[g], {"tp": tp_at(2 * d)}
            ).start()

    def soften(g, found):
        mine = slice(g * sg, (g + 1) * sg)
        own_score = (
            by_head(
                [
                    jnp.sum(
                        jnp.where(lane_head == h, query[mine] * key_new[mine], 0.0),
                        axis=1,
                        keepdims=True,
                    )
                    for h in range(heads)
                ]
            )
            * scale
        )
        full = found * scale + gate_rows[g * grows : (g + 1) * grows, :]
        largest = jnp.maximum(jnp.max(full, axis=1, keepdims=True), own_score)
        past = jnp.exp(full - largest)
        own_term = jnp.exp(own_score - largest)
        total = jnp.sum(past, axis=1, keepdims=True) + own_term
        return past / total, (own_term / total).astype(BF16).astype(F32)

    found = score(0)
    pl.semaphore_wait(relay.at[len(bits) - 1], 1)
    key_new = projected(1)
    value_new = projected(2)
    for load in value_loads:
        load.wait()
    loads[3].wait()
    softened = []
    for g in range(SEQ_GROUPS):
        later = score(g + 1) if g + 1 < SEQ_GROUPS else None
        softened.append(soften(g, found))
        found = later
    for g in range(SEQ_GROUPS):
        mine = slice(g * sg, (g + 1) * sg)
        past_weights, own_weight = softened[g]
        gathered = jnp.zeros((grows, cols), F32)
        for s in range(sg):
            chosen = jnp.where(group_seq == s, past_weights, 0.0).astype(BF16)
            gathered = gathered + matmul(chosen, values[g * sg + s])
        attended = jnp.zeros((sg, cols), F32)
        for h in range(heads):
            part = slice(h * sg, (h + 1) * sg)
            attended = jnp.where(
                lane_head == h, gathered[part] + own_weight[part] * value_new[mine], attended
            )
        attended = attended.astype(BF16)
        if g:
            finish_pair(g - 1)

        def outward(c):
            return jnp.concatenate(
                [
                    matmul(
                        attended,
                        wo[:, pl.ds(pl.multiple_of((2 * t + c) * slice_w, slice_w), slice_w)],
                    )
                    for t in range(levels)
                ],
                axis=1,
            )

        pair_send[g] = outward(1 - core).astype(BF16)
        last = 2 * (levels - 1)
        remote(
            pair_send.at[g], zfar_recv.at[g, 1], zfar_ss, zfar_rs.at[g], {"tp": tp_at(last + 1)}
        ).start()
        remote(
            pair_send.at[g], pair_recv.at[g], pair_ss, pair_rs.at[g], {"tp": tp_at(1)}
        ).start()
        own_part[g] = outward(core)
        zfar_send[g] = own_part[g].astype(BF16)
        remote(
            zfar_send.at[g], zfar_recv.at[g, 0], zfar_ss, zfar_rs.at[g], {"tp": tp_at(last)}
        ).start()
    def transposed(src, dst, low, high):
        @pl.loop(low, high)
        def _(t):
            into = lax.rem(t, 2) * half_w + lax.div(t, 2) * slice_w
            dst[pl.ds(pl.multiple_of(into, slice_w), slice_w), :] = src[
                :, pl.ds(pl.multiple_of(t * slice_w, slice_w), slice_w)
            ].T

    loads[4].wait()
    loads[5].wait()
    transposed(wg, wg_t, 0, n_tp // 2)
    finish_pair(SEQ_GROUPS - 1)
    transposed(wg, wg_t, n_tp // 2, n_tp)
    transposed(wu, wu_t, 0, n_tp)

    stream_half = jnp.concatenate(
        [
            stream[:, pl.ds(pl.multiple_of((2 * t + core) * slice_w, slice_w), slice_w)]
            for t in range(levels)
        ],
        axis=1,
    ).astype(F32)

    for g in range(SEQ_GROUPS):
        total = stream_half[g * sg : (g + 1) * sg] + zs_send[g].astype(F32)
        wait_all(zs_recv.at[g, pl.ds(1, levels - 2)], zs_rs.at[g])
        for d in range(1, levels - 1):
            total = total + zs_recv[g, d].astype(F32)
        wait_all(zfar_recv.at[g], zfar_rs.at[g])
        total = total + zfar_recv[g, 0].astype(F32) + zfar_recv[g, 1].astype(F32)
        mix[core, my_ep, g] = total.astype(BF16)
        here = mix.at[core, my_ep, g]
        for k in reversed(range(n_ep)):
            for c in range(2):
                if k or c:
                    remote(
                        here,
                        here,
                        mix_ss.at[c],
                        mix_rs.at[c],
                        {"ep": ep_at(k), "tp": tp_at(c)},
                    ).start()

    share = jnp.sum(
        jnp.where(routes[...] == my_ep, route_weights[...], 0.0), axis=0, keepdims=True
    )
    square = (tokens, tokens)
    diagonal = lax.broadcasted_iota(jnp.int32, square, 0) == lax.broadcasted_iota(
        jnp.int32, square, 1
    )
    coefficient = jnp.sum(jnp.where(diagonal, share, 0.0), axis=1, keepdims=True)
    loads[6].wait()
    wait_all(mix.at[0, others], mix_rs.at[0])
    wait_all(mix.at[1], mix_rs.at[1])
    halves = [mix[c].astype(F32).reshape(tokens, half_w) for c in range(2)]
    squares = sum(jnp.sum(half * half, axis=1, keepdims=True) for half in halves)
    inverse = lax.rsqrt(squares / width + 1e-06)
    normed_ffn = jnp.concatenate(
        [
            (
                halves[c]
                * inverse
                * jnp.concatenate(
                    [
                        gain_ffn[:, (2 * t + c) * slice_w : (2 * t + c + 1) * slice_w]
                        for t in range(levels)
                    ],
                    axis=1,
                )
            ).astype(BF16)
            for c in range(2)
        ],
        axis=1,
    )
    gate = matmul(normed_ffn, wg_t[...])
    up = matmul(normed_ffn, wu_t[...])
    hidden = (gate / (1.0 + jnp.exp(-gate)) * up).astype(BF16)

    def downward(c, d):
        at = (2 * flip(level, d) + c) * slice_w
        return matmul(hidden, wd[:, pl.ds(pl.multiple_of(at, slice_w), slice_w)]) * coefficient

    for d in reversed(range(levels)):
        dpair_send[d] = downward(1 - core, d).astype(BF16)
        remote(
            dpair_send.at[d], dpair_recv.at[d], dpair_ss, dpair_rs.at[d], {"tp": tp_at(1)}
        ).start()
    for d in range(levels):
        down_part[d] = downward(core, d)
    for d in reversed(range(levels)):
        wait_all(dpair_recv.at[d], dpair_rs.at[d])
        summed = down_part[d] + dpair_recv[d].astype(F32)
        for e in range(n_ep):
            fs_send[d, e] = summed[e * seqs : (e + 1) * seqs].astype(BF16)
        near = min(1, d)
        for k in reversed(range(n_ep)):
            if d or k:
                remote(
                    fs_send.at[d, ep_at(k)],
                    fs_recv.at[d, k],
                    fs_ss.at[near],
                    fs_rs.at[near],
                    {"ep": ep_at(k), "tp": tp_at(2 * d)},
                ).start()
    own_stream = mix[
        core, my_ep, :, :, pl.ds(pl.multiple_of(level * slice_w, slice_w), slice_w)
    ].astype(F32).reshape(seqs, slice_w)
    combined = own_stream + fs_send[0, my_ep].astype(F32)
    far = pl.ds(1, levels - 1)
    wait_all(fs_recv.at[far], fs_rs.at[1])
    wait_all(fs_recv.at[0, others], fs_rs.at[0])
    for d in range(levels):
        for k in range(n_ep):
            if d or k:
                combined = combined + fs_recv[d, k].astype(F32)
    out[...] = combined.astype(BF16)
    wait_all(a2a_send.at[others], a2a_ss)
    wait_all(part_recv.at[:, others], part_ss)
    wait_all(pair_send, pair_ss)
    wait_all(zs_recv.at[:, pl.ds(1, levels - 2)], zs_ss)
    wait_all(zfar_recv, zfar_ss)
    wait_all(mix.at[0, others], mix_ss.at[0])
    wait_all(mix.at[1], mix_ss.at[1])
    wait_all(dpair_send, dpair_ss)
    wait_all(fs_recv.at[far], fs_ss.at[1])
    wait_all(fs_recv.at[0, others], fs_ss.at[0])


def shards(
    stream,
    norm_gain_attn,
    w_query,
    w_key,
    w_value,
    w_forget,
    forget_bias,
    key_cache,
    value_cache,
    gate_cache,
    lengths,
    w_output,
    norm_gain_ffn,
    routes,
    route_weights,
    w_expert_gate,
    w_expert_up,
    expert_down_weight,
):
    n_ep = lax.axis_size("ep")
    n_tp = lax.axis_size("tp")
    seqs, width = stream.shape
    heads = gate_cache.shape[1]
    cache = key_cache.shape[1]
    depth, cols = w_query.shape
    hidden = w_expert_gate.shape[2]
    padded = -(-hidden // LANES) * LANES
    slice_w = width // n_tp
    levels = n_tp // 2
    half_w = levels * slice_w
    rows = heads * seqs
    sg = seqs // SEQ_GROUPS
    vmem = pl.BlockSpec(memory_space=pltpu.VMEM)
    hbm = pl.BlockSpec(memory_space=pltpu.HBM)
    dma = pltpu.SemaphoreType.DMA
    small = (
        stream,
        norm_gain_attn[None, :],
        w_forget.T,
        forget_bias[None, :],
        gate_cache,
        lengths[None, :],
        norm_gain_ffn[None, :],
        routes.T,
        route_weights.T,
    )
    return pl.pallas_call(
        functools.partial(layer_kernel, n_ep, n_tp, heads),
        out_shape=jax.ShapeDtypeStruct((seqs, slice_w), BF16),
        in_specs=[hbm] * 18,
        out_specs=vmem,
        scratch_shapes=[pltpu.VMEM(array.shape, array.dtype) for array in small]
        + [
            pltpu.VMEM((3, depth, cols), BF16),
            pltpu.VMEM((seqs, cache, cols), BF16),
            pltpu.VMEM((seqs * cols, cache), BF16),
            pltpu.VMEM((seqs, cache, cols), BF16),
            pltpu.VMEM((cols, width), BF16),
            pltpu.VMEM((padded, width), BF16),
            pltpu.VMEM((padded, width), BF16),
            pltpu.VMEM((padded, width), BF16),
            pltpu.VMEM((width, padded), BF16),
            pltpu.VMEM((width, padded), BF16),
            pltpu.VMEM((n_ep, seqs, depth), BF16),
            pltpu.VMEM((n_ep, seqs, depth), BF16),
            pltpu.VMEM((3, n_ep, seqs, cols), F32),
            pltpu.VMEM((3, n_ep, seqs, cols), F32),
            pltpu.VMEM((rows, cache), F32),
            pltpu.VMEM((SEQ_GROUPS, sg, half_w), BF16),
            pltpu.VMEM((SEQ_GROUPS, sg, half_w), BF16),
            pltpu.VMEM((SEQ_GROUPS, sg, half_w), F32),
            pltpu.VMEM((SEQ_GROUPS, sg, half_w), BF16),
            pltpu.VMEM((SEQ_GROUPS, levels, sg, half_w), BF16),
            pltpu.VMEM((SEQ_GROUPS, sg, half_w), BF16),
            pltpu.VMEM((SEQ_GROUPS, 2, sg, half_w), BF16),
            pltpu.VMEM((2, n_ep, SEQ_GROUPS, sg, half_w), BF16),
            pltpu.VMEM((levels, n_ep * seqs, slice_w), BF16),
            pltpu.VMEM((levels, n_ep * seqs, slice_w), BF16),
            pltpu.VMEM((levels, n_ep * seqs, slice_w), F32),
            pltpu.VMEM((levels, n_ep, seqs, slice_w), BF16),
            pltpu.VMEM((levels, n_ep, seqs, slice_w), BF16),
            dma((len(small),)),
            dma((7,)),
            dma((CACHE_LOADS,)),
            dma((CACHE_LOADS,)),
            pltpu.SemaphoreType.REGULAR((levels.bit_length() - 1,)),
            dma,
            dma,
            dma,
            dma((3,)),
            dma,
            dma((SEQ_GROUPS,)),
            dma,
            dma((SEQ_GROUPS,)),
            dma,
            dma((SEQ_GROUPS,)),
            dma((2,)),
            dma((2,)),
            dma,
            dma((levels,)),
            dma((2,)),
            dma((2,)),
        ],
        compiler_params=pltpu.CompilerParams(
            collective_id=0, has_side_effects=True, vmem_limit_bytes=48 * 1024 * 1024
        ),
    )(
        *(
            pltpu.with_memory_space_constraint(array, pltpu.HBM)
            for array in (
                *small,
                w_query,
                w_key,
                w_value,
                key_cache,
                value_cache,
                w_output,
                jnp.swapaxes(w_expert_gate, 1, 2),
                jnp.swapaxes(w_expert_up, 1, 2),
                expert_down_weight,
            )
        )
    )


def solution(mesh):
    placed = (
        P("ep", None),
        P(),
        P("ep", "tp"),
        P("ep", "tp"),
        P("ep", "tp"),
        P(),
        P(),
        P("ep", None, "tp"),
        P("ep", None, "tp"),
        P("ep", "tp", None),
        P("ep"),
        P("tp", None),
        P(),
        P(),
        P(),
        P("ep", None, "tp"),
        P("ep", None, "tp"),
        P("ep", "tp", None),
    )
    return jax.shard_map(
        shards, mesh=mesh, in_specs=placed, out_specs=P("ep", "tp"), check_vma=False
    )
```
